128 devices in a mesh: kv: 16 (over z, y), tp: 8 (over x, core).
Axes of the slice: x: 4, y: 4, z: 4, core: 2. Of those that a mesh axis runs over, the one named last changes fastest.
Arguments:
- tokens: bfloat16 [32, 4096], P(None, ('kv', 'tp')), may hold values from -36 to 36
- first_gain: float32 [4096], P('kv'), may hold values from 0.1 to 1.9
- first_gate: bfloat16 [4096, 11264], P('kv', 'tp'), may hold values from -0.09375 to 0.09375
- first_up: bfloat16 [4096, 11264], P('kv', 'tp'), may hold values from -0.09375 to 0.09375
- first_down: bfloat16 [11264, 4096], P('tp', 'kv'), may hold values from -0.0546875 to 0.0546875
- mix_gain: float32 [4096], P('kv'), may hold values from 0.1 to 1.9
- w_query: bfloat16 [4096, 2048], P('kv', 'tp'), may hold values from -0.09375 to 0.09375
- key_cache: bfloat16 [32, 16384, 1024], P(None, 'kv', 'tp'), may hold values from -100 to 100
- value_cache: bfloat16 [32, 16384, 1024], P(None, 'kv', 'tp'), may hold values from -6 to 6
- map_weight: float32 [32], P('tp'), may hold values from 0.3 to 0.8
- head_gain: float32 [64], replicated, may hold values from 0.1 to 1.9
- w_out: bfloat16 [2048, 4096], P('tp', 'kv'), may hold values from -0.125 to 0.125
- second_gain: float32 [4096], P('kv'), may hold values from 0.1 to 1.9
- second_gate: bfloat16 [4096, 11264], P('kv', 'tp'), may hold values from -0.09375 to 0.09375
- second_up: bfloat16 [4096, 11264], P('kv', 'tp'), may hold values from -0.09375 to 0.09375
- second_down: bfloat16 [11264, 4096], P('tp', 'kv'), may hold values from -0.0546875 to 0.0546875
Outputs:
- mixed: bfloat16 [32, 4096], P(None, ('kv', 'tp'))
The draws below stay inside these ranges and needn't reach their ends.
All inputs are finite; a program needn't handle non-finite values.
Results may differ from the reference program's by a relative error of at most 0.0158.
Values may be sent and summed in bfloat16 or wider, within the bound.
A program may use at most 128 MiB of HBM per device.

```python
import math
import jax
import jax.numpy as jnp
from jax import lax

D = 4096
FF = 11264
HEADS = 32
KV_HEADS = 16
HEAD = 64
HALF = 32
BATCH = 32
LENGTH = 16384
DKV = 256


def draw_tokens(key, part):
    columns = jnp.arange(D, dtype=jnp.float32)
    inner = jnp.arange(D, dtype=jnp.int32) % DKV
    col_scale = 3.0 ** (columns / D - 0.5) * 3.0 ** (inner.astype(jnp.float32) / DKV - 0.5)
    row_scale = jnp.exp(jax.random.uniform(jax.random.fold_in(key, 1), (BATCH, 1), jnp.float32, math.log(0.3), math.log(3.0)))
    entries = jnp.clip(jax.random.normal(jax.random.fold_in(key, 2), (BATCH, D), jnp.float32), -4.0, 4.0)
    return (entries * row_scale * col_scale[None, :]).astype(jnp.bfloat16)


def draw_key_cache(key, part):
    width = KV_HEADS * HEAD
    base = jnp.clip(jax.random.normal(jax.random.fold_in(key, 11), (BATCH, LENGTH, width), jnp.float32), -6.0, 6.0) * 1.75
    return base.astype(jnp.bfloat16)


def shard_levels(key, dims, pieces, smallest, largest):
    level, own = 1.0, jax.random.fold_in(key, 6)
    for dim, blocks in pieces:
        draws = jnp.exp(jax.random.uniform(jax.random.fold_in(own, dim), (blocks,), jnp.float32, smallest / len(pieces), largest / len(pieces)))
        level = level * jnp.repeat(draws, dims[dim] // blocks).reshape([-1 if axis == dim else 1 for axis in range(len(dims))])
    return level


def scatter_about(key, extent, deviation, most, shards=(), kind=jnp.bfloat16):
    array = deviation * jax.random.normal(key, extent, jnp.float32)
    if shards:
        array = array * shard_levels(key, extent, shards, -0.22, 0.18)
    return jnp.clip(array, -most, most).astype(kind)


def setup_inputs(seed: int = 0) -> dict:
    streams_of = jax.random.split(jax.random.key(seed), 17)
    tokens = draw_tokens(jax.random.fold_in(streams_of[16], 71), 0)
    first_gain = jnp.clip(1.0 + 0.18 * jax.random.normal(streams_of[1], (D,), jnp.float32), 0.1, 1.9)
    first_gate = scatter_about(streams_of[2], (D, FF), D ** -0.5, 0.09375, ((0, 16), (1, 8)))
    first_up = scatter_about(streams_of[3], (D, FF), D ** -0.5, 0.09375, ((0, 16), (1, 8)))
    first_down = scatter_about(streams_of[4], (FF, D), FF ** -0.5, 0.0546875, ((0, 8), (1, 16)))
    mix_gain = jnp.clip(1.0 + 0.18 * jax.random.normal(streams_of[5], (D,), jnp.float32), 0.1, 1.9)
    w_query = scatter_about(streams_of[6], (D, HEADS * HEAD), D ** -0.5, 0.09375, ((0, 16), (1, 8)))
    key_cache = draw_key_cache(jax.random.fold_in(streams_of[16], 71), 0)
    value_cache = scatter_about(streams_of[8], (BATCH, LENGTH, KV_HEADS * HEAD), 1.0, 6.0, ((1, 16), (2, 8)))
    map_weight = jnp.clip(0.3 + 0.5 * jax.random.uniform(streams_of[9], (HEADS,), jnp.float32) ** shard_levels(streams_of[9], (HEADS,), ((0, 8),), -0.2, 0.2), 0.3, 0.8)
    head_gain = jnp.clip(1.0 + 0.18 * jax.random.normal(streams_of[10], (HEAD,), jnp.float32), 0.1, 1.9)
    w_out = scatter_about(streams_of[11], (HEADS * HEAD, D), (HEADS * HEAD) ** -0.5, 0.125, ((0, 8), (1, 16)))
    second_gain = jnp.clip(1.0 + 0.18 * jax.random.normal(streams_of[12], (D,), jnp.float32), 0.1, 1.9)
    second_gate = scatter_about(streams_of[13], (D, FF), D ** -0.5, 0.09375, ((0, 16), (1, 8)))
    second_up = scatter_about(streams_of[14], (D, FF), D ** -0.5, 0.09375, ((0, 16), (1, 8)))
    second_down = scatter_about(streams_of[15], (FF, D), FF ** -0.5, 0.0546875, ((0, 8), (1, 16)))
    return dict(tokens=tokens, first_gain=first_gain, first_gate=first_gate, first_up=first_up, first_down=first_down, mix_gain=mix_gain, w_query=w_query, key_cache=key_cache, value_cache=value_cache, map_weight=map_weight, head_gain=head_gain, w_out=w_out, second_gain=second_gain, second_gate=second_gate, second_up=second_up, second_down=second_down)


EPS = 1e-06
HEAD_SCALE = 0.8

def channel_mixer(residual, gain, w_gate, w_up, w_down):
    factor = lax.rsqrt(lax.optimization_barrier(jnp.mean(residual * residual, axis=1, keepdims=True)) + EPS)
    scaled = (residual * gain).astype(jnp.bfloat16)
    gate_sum = factor * jnp.dot(scaled, w_gate, preferred_element_type=jnp.float32)
    up_sum = factor * jnp.dot(scaled, w_up, preferred_element_type=jnp.float32)
    active = (jax.nn.silu(gate_sum) * up_sum).astype(jnp.bfloat16)
    return jnp.dot(active, w_down, preferred_element_type=jnp.float32)

def attention_mix(residual, mix_gain, w_query, key_cache, value_cache, map_weight, head_gain, w_out):
    factor = lax.rsqrt(lax.optimization_barrier(jnp.mean(residual * residual, axis=1, keepdims=True)) + EPS)
    scaled = (residual * mix_gain).astype(jnp.bfloat16)
    queries = (factor * jnp.dot(scaled, w_query, preferred_element_type=jnp.float32)).astype(jnp.bfloat16)
    group = HEADS // KV_HEADS

    def one_row(items):
        row_query, row_keys, row_values = items
        query_full = row_query.astype(jnp.float32).reshape(KV_HEADS, group, HEAD)
        keys_full = row_keys.astype(jnp.float32).reshape(-1, KV_HEADS, HEAD)
        values_full = row_values.astype(jnp.float32).reshape(-1, KV_HEADS, HEAD)

        def one_map(first_col, last_col):
            scores = jnp.einsum('kgd,pkd->kgp', query_full[..., first_col:last_col], keys_full[..., first_col:last_col]) / math.sqrt(last_col - first_col)
            row_peak = lax.optimization_barrier(jnp.max(scores, axis=2, keepdims=True))
            exp_terms = jnp.exp(scores - row_peak)
            weights_sum = lax.optimization_barrier(jnp.sum(exp_terms, axis=2))
            rounded = lax.optimization_barrier(exp_terms.astype(jnp.bfloat16)).astype(jnp.float32)
            return jnp.einsum('kgp,pkd->kgd', rounded, values_full) / weights_sum[..., None]
        return (one_map(0, HALF), one_map(HALF, HEAD))
    out_one, out_two = lax.map(one_row, (queries, key_cache, value_cache))
    combined = out_one - map_weight.reshape(KV_HEADS, group)[..., None] * out_two
    normed = combined * lax.rsqrt(lax.optimization_barrier(jnp.mean(combined * combined, axis=3, keepdims=True)) + EPS) * head_gain * HEAD_SCALE
    normed = normed.astype(jnp.bfloat16).reshape(BATCH, HEADS * HEAD)
    return jnp.dot(normed, w_out, preferred_element_type=jnp.float32)

def reference(tokens, first_gain, first_gate, first_up, first_down, mix_gain, w_query, key_cache, value_cache, map_weight, head_gain, w_out, second_gain, second_gate, second_up, second_down):
    residual = tokens.astype(jnp.float32)
    residual = residual + 0.5 * channel_mixer(residual, first_gain, first_gate, first_up, first_down)
    residual = residual + attention_mix(residual, mix_gain, w_query, key_cache, value_cache, map_weight, head_gain, w_out)
    residual = residual + 0.5 * channel_mixer(residual, second_gain, second_gate, second_up, second_down)
    return residual.astype(jnp.bfloat16)
```

```python
import functools
import math

import jax
import jax.numpy as jnp
from jax import lax
from jax.experimental import pallas as pl
from jax.experimental.pallas import tpu as pltpu
from jax.sharding import PartitionSpec as P

HEAD = 64
MAPS = 2
LANES = 128
TILE = 8
EPS = 1e-06
HEAD_SCALE = 0.8
SIDE = 4
ROW_GROUPS = 4
COL_GROUPS = 4
F32 = jnp.float32
BF16 = jnp.bfloat16
MESH = pl.DeviceIdType.MESH
VMEM_LIMIT = 60 * 1024 * 1024


def hops(d):
    return min(d, SIDE - d)


def kv_offsets():
    offs = [(a, b) for a in range(SIDE) for b in range(SIDE) if (a, b) != (0, 0)]
    return sorted(offs, key=lambda o: -(hops(o[0]) + hops(o[1])))


def tp_offsets():
    offs = [(a, b) for a in range(SIDE) for b in range(2) if (a, b) != (0, 0)]
    return sorted(offs, key=lambda o: -(2 * hops(o[0]) + o[1]))


def shifted(axis, offset):
    me = lax.axis_index(axis)
    inner = SIDE if axis == "kv" else 2
    high = lax.rem(me // inner + offset[0], SIDE)
    low = lax.rem(lax.rem(me, inner) + offset[1], inner)
    return high * inner + low


OFFSETS = {"kv": kv_offsets(), "tp": tp_offsets()}


def greet():
    barrier = pltpu.get_barrier_semaphore()
    total = 0
    for axis in ("kv", "tp"):
        for offset in OFFSETS[axis]:
            pl.semaphore_signal(
                barrier, inc=1, device_id={axis: shifted(axis, offset)}, device_id_type=MESH
            )
            total += 1
    pl.semaphore_wait(barrier, total)


def exchange(axis, source, target, sems):
    copies = []
    for k, offset in enumerate(OFFSETS[axis]):
        dest = shifted(axis, offset)
        copy = pltpu.make_async_remote_copy(
            src_ref=source(dest),
            dst_ref=target(k),
            send_sem=sems.at[0, k],
            recv_sem=sems.at[1, k],
            device_id={axis: dest},
            device_id_type=MESH,
        )
        copy.start()
        copies.append(copy)
    return copies


def total_of(copies, own, recv):
    total = own
    for k in reversed(range(len(copies))):
        copies[k].wait()
        total = total + recv[k].astype(F32)
    return total


def dot(a, b):
    return jnp.dot(a, b, preferred_element_type=F32)


def row_squares(h):
    return jnp.sum(h * h, axis=1, keepdims=True)


def squares_tile(h):
    s = row_squares(h)
    high = s.astype(BF16).astype(F32)
    lane = lax.broadcasted_iota(jnp.int32, (h.shape[0], LANES), 1)
    return jnp.where(lane < LANES // 2, high, s - high).astype(BF16)


def row_factor(tile, width):
    s = tile[:, :1] + tile[:, LANES // 2 : LANES // 2 + 1]
    return lax.rsqrt(s / width + EPS)


def feed_forward(n_kv, h, gain, w_gate, w_up, w_down, loads, scratch):
    send, recv, act_own, act_all, rs_sems, ag_sems = scratch
    me = lax.axis_index("kv")
    hidden = w_gate.shape[1]
    cw = act_own.shape[1]
    tile = squares_tile(h)
    scaled = (h * gain).astype(BF16)
    loads[0].wait()
    loads[1].wait()
    for c in range(COL_GROUPS):
        low = c * cw
        w = min(cw, hidden - low)
        for base, weight in ((0, w_gate), (cw, w_up)):
            part = dot(scaled, weight[:, low : low + w])
            for r in range(ROW_GROUPS):
                rows = slice(r * TILE, (r + 1) * TILE)
                send[r * COL_GROUPS + c, :, base : base + w] = part[rows].astype(BF16)
                if w < cw:
                    send[r * COL_GROUPS + c, :, base + w : base + cw] = jnp.zeros(
                        (TILE, cw - w), BF16
                    )
        for r in range(ROW_GROUPS):
            send[r * COL_GROUPS + c, :, 2 * cw :] = tile[r * TILE : (r + 1) * TILE]
    copies = exchange("kv", lambda d: send.at[d], lambda k: recv.at[k], rs_sems)
    total = total_of(copies, send[me].astype(F32), recv)
    factor = row_factor(total[:, 2 * cw :], h.shape[1] * n_kv)
    gate = total[:, :cw] * factor
    up = total[:, cw : 2 * cw] * factor
    act = (gate / (1.0 + jnp.exp(-gate)) * up).astype(BF16)
    act_own[...] = act
    act_all[me] = act
    copies = exchange("kv", lambda d: act_own, lambda k: act_all.at[me], ag_sems)
    for copy in copies:
        copy.wait()
    loads[2].wait()
    out = None
    for c in range(COL_GROUPS):
        low = c * cw
        w = min(cw, hidden - low)
        block = jnp.concatenate(
            [act_all[r * COL_GROUPS + c, :, :w].astype(F32) for r in range(ROW_GROUPS)], axis=0
        ).astype(BF16)
        term = dot(block, w_down[low : low + w, :])
        out = term if out is None else out + term
    return out


def sum_over_tp(part, send, recv, sems):
    send[...] = part.astype(BF16)
    copies = exchange("tp", lambda d: send, lambda k: recv.at[k], sems)
    return total_of(copies, send[...].astype(F32), recv)


def query_step(n_kv, h, gain, w_query, q_send, q_recv, q_sems):
    rows = h.shape[0]
    product = dot((h * gain).astype(BF16), w_query[...])
    row = lax.broadcasted_iota(jnp.int32, (rows, LANES), 0)
    lane = lax.broadcasted_iota(jnp.int32, (rows, LANES), 1)
    s = jnp.sum(jnp.where(row == lane, row_squares(h), 0.0), axis=0, keepdims=True)
    high = s.astype(BF16).astype(F32)
    first = lax.broadcasted_iota(jnp.int32, (TILE, LANES), 0)
    stats = jnp.where(first == 0, high, jnp.where(first == 1, s - high, 0.0))
    tiles = rows // TILE
    for r in range(tiles):
        for c in range(2):
            q_send[2 * r + c] = product[
                r * TILE : (r + 1) * TILE, c * LANES : (c + 1) * LANES
            ].astype(BF16)
    q_send[2 * tiles] = stats.astype(BF16)
    copies = exchange("kv", lambda d: q_send, lambda k: q_recv.at[k], q_sems)
    total = total_of(copies, q_send[...].astype(F32), q_recv)
    s = jnp.sum(total[2 * tiles], axis=0, keepdims=True)
    factor = lax.rsqrt(s / (h.shape[1] * n_kv) + EPS)
    factor = jnp.sum(jnp.where(row == lane, factor, 0.0), axis=1, keepdims=True)
    halves = [
        jnp.concatenate([total[2 * r + c] for r in range(tiles)], axis=0) * factor
        for c in range(2)
    ]
    low = lane < HEAD
    first_half = jnp.where(low, halves[0], pltpu.roll(halves[1], HEAD, 1))
    second_half = jnp.where(low, pltpu.roll(halves[0], HEAD, 1), halves[1])
    return first_half.astype(BF16), second_half.astype(BF16)


def spread_queries(q_parts, pairs, qx):
    batch = q_parts[0].shape[0]
    per = qx.shape[1]
    rows = pairs * per
    row = lax.broadcasted_iota(jnp.int32, (rows, batch), 0)
    col = lax.broadcasted_iota(jnp.int32, (rows, batch), 1)
    pick = jnp.where(col == row // per + pairs * lax.rem(row, 2), 1.0, 0.0).astype(BF16)
    wide_row = lax.broadcasted_iota(jnp.int32, (rows, LANES), 0)
    lane = lax.broadcasted_iota(jnp.int32, (rows, LANES), 1)
    which = lax.rem(wide_row // 2, 2)
    y = jnp.where(which == 0, dot(pick, q_parts[0]), dot(pick, q_parts[1]))
    mine = lane // (HEAD // MAPS) == lax.rem(wide_row // 4, 4)
    y = jnp.where(mine, y, 0.0)
    member = lax.rem(wide_row, 2)
    for i in range(2):
        block = jnp.where(member == i, y, 0.0).astype(BF16)
        qx[:, :, i * LANES : (i + 1) * LANES] = block.reshape(pairs, per, LANES)


def attend(scale, qx, k_buf, v_buf, p, o_ref, slot):
    s = lax.dot_general(qx[p], k_buf[p], (((1,), (1,)), ((), ())), preferred_element_type=F32)
    peak = jnp.max(s, axis=1, keepdims=True)
    e = jnp.exp2((s - peak) * scale)
    l = jnp.sum(e, axis=1, keepdims=True)
    o = dot(e.astype(BF16), v_buf[p]) / l
    lse = peak * scale + jnp.log2(l)
    row = lax.broadcasted_iota(jnp.int32, (2 * TILE, LANES), 0)
    lane = lax.broadcasted_iota(jnp.int32, (TILE, LANES), 1)
    o = jnp.where(lax.rem(row, 2) == 0, o[:, :LANES], o[:, LANES:])
    low = lane < HEAD
    o_ref[slot, 0] = jnp.where(low, o[:TILE], o[TILE:])
    o_ref[slot, 1] = jnp.where(low, lse[:TILE], lse[TILE:])


def attention_step(scale, n_kv, qx, k_buf, v_buf, o_send, o_recv, sems):
    order = OFFSETS["kv"]
    copies = []
    for k, offset in enumerate(order):
        dest = shifted("kv", offset)
        attend(scale, qx, k_buf, v_buf, dest, o_send, k)
        copy = pltpu.make_async_remote_copy(
            src_ref=o_send.at[k],
            dst_ref=o_recv.at[k],
            send_sem=sems.at[0, k],
            recv_sem=sems.at[1, k],
            device_id={"kv": dest},
            device_id_type=MESH,
        )
        copy.start()
        copies.append(copy)
    attend(scale, qx, k_buf, v_buf, lax.axis_index("kv"), o_send, len(order))
    return copies


def merge_heads(copies, o_send, o_recv, map_weight, head_gain, group, kv_local):
    for copy in copies:
        copy.wait()
    own = len(copies)
    outs = [o_send[own, 0]] + [o_recv[k, 0] for k in range(own)]
    lses = [o_send[own, 1]] + [o_recv[k, 1] for k in range(own)]
    peak = functools.reduce(jnp.maximum, lses)
    weights = [jnp.exp2(lse - peak) for lse in lses]
    total = functools.reduce(jnp.add, weights)
    merged = functools.reduce(jnp.add, [w * o for w, o in zip(weights, outs)]) / total
    row = lax.broadcasted_iota(jnp.int32, (TILE, LANES), 0)
    lane = lax.broadcasted_iota(jnp.int32, (TILE, LANES), 1)
    weight = jnp.zeros((TILE, LANES), F32)
    for k in range(kv_local):
        for g in range(group):
            here = (lax.rem(row // 2, group) == g) & (lane // HEAD == k)
            at = k * group + g
            weight = jnp.where(here, map_weight[:, at : at + 1], weight)
    diff = merged - weight * pltpu.roll(merged, TILE // 2, 0)
    square = diff * diff
    mean = jnp.zeros((TILE, LANES), F32)
    for k in range(kv_local):
        here = lane // HEAD == k
        mean = jnp.where(here, jnp.sum(jnp.where(here, square, 0.0), axis=1, keepdims=True), mean)
    gain = jnp.concatenate([head_gain[...]] * kv_local, axis=1)
    return diff * lax.rsqrt(mean / HEAD + EPS) * gain * HEAD_SCALE


def start_loads(pairs, sems):
    loads = [pltpu.make_async_copy(a, b, sems.at[i]) for i, (a, b) in enumerate(pairs)]
    for load in loads:
        load.start()
    return loads


def layer_kernel(
    n_kv, n_tp, kv_local, group, scale,
    tokens, first_gain, mix_gain, second_gain, map_weight, head_gain,
    gate1_any, up1_any, down1_any, query_any, key_any, value_any, out_any,
    gate2_any, up2_any, down2_any,
    mixed,
    w_gate1, w_up1, w_down1, w_query, k_buf, v_buf, w_out, w_gate2, w_up2, w_down2,
    tok_all, rs1_send, rs1_recv, act1_own, act1_all, tp1_send, tp1_recv, q_send, q_recv, qx,
    o_send, o_recv, head_own, head_all, tp2_send, tp2_recv,
    rs2_send, rs2_recv, act2_own, act2_all, fin_send, fin_recv,
    load_sems, tok_sems, rs1_sems, ag1_sems, tp1_sems, q_sems, o_sems, head_sems, tp2_sems,
    rs2_sems, ag2_sems, fin_sems,
):
    pairs = k_buf.shape[0]
    chunk = HEAD
    loads = start_loads(
        (
            (gate1_any, w_gate1),
            (up1_any, w_up1),
            (down1_any, w_down1),
            (query_any, w_query),
            (key_any.at[:pairs], k_buf.at[:, :, :LANES]),
            (key_any.at[pairs:], k_buf.at[:, :, LANES:]),
            (value_any.at[:pairs], v_buf.at[:, :, :LANES]),
            (value_any.at[pairs:], v_buf.at[:, :, LANES:]),
            (gate2_any, w_gate2),
            (up2_any, w_up2),
            (down2_any, w_down2),
        )
        + tuple(
            (
                out_any.at[pl.ds((k * group + g) * chunk, chunk)],
                w_out.at[pl.ds((g * kv_local + k) * chunk, chunk)],
            )
            for k in range(kv_local)
            for g in range(group)
        ),
        load_sems,
    )
    greet()
    tp = lax.axis_index("tp")
    me = lax.axis_index("kv")
    tok_all[tp] = tokens[...]
    for copy in exchange("tp", lambda d: tokens, lambda k: tok_all.at[tp], tok_sems):
        copy.wait()
    h = jnp.concatenate([tok_all[j].astype(F32) for j in range(n_tp)], axis=1)
    part = feed_forward(
        n_kv, h, first_gain[...], w_gate1, w_up1, w_down1, loads[:3],
        (rs1_send, rs1_recv, act1_own, act1_all, rs1_sems, ag1_sems),
    )
    h = h + 0.5 * sum_over_tp(part, tp1_send, tp1_recv, tp1_sems)
    loads[3].wait()
    q_parts = query_step(n_kv, h, mix_gain[...], w_query, q_send, q_recv, q_sems)
    spread_queries(q_parts, pairs, qx)
    for load in loads[4:8]:
        load.wait()
    copies = attention_step(scale, n_kv, qx, k_buf, v_buf, o_send, o_recv, o_sems)
    heads = merge_heads(copies, o_send, o_recv, map_weight, head_gain, group, kv_local)
    head_own[...] = heads
    mine = pl.ds(pl.multiple_of(me * TILE, TILE), TILE)
    head_all[mine, :] = heads
    for copy in exchange("kv", lambda d: head_own, lambda k: head_all.at[mine], head_sems):
        copy.wait()
    heads = jnp.concatenate(
        [
            jnp.concatenate(
                [head_all[pl.ds(2 * g + i, pairs, stride=TILE), :] for g in range(group)], axis=1
            )
            for i in range(2)
        ],
        axis=0,
    ).astype(BF16)
    for load in loads[11:]:
        load.wait()
    h = h + sum_over_tp(dot(heads, w_out[...]), tp2_send, tp2_recv, tp2_sems)
    part = feed_forward(
        n_kv, h, second_gain[...], w_gate2, w_up2, w_down2, loads[8:11],
        (rs2_send, rs2_recv, act2_own, act2_all, rs2_sems, ag2_sems),
    )
    batch, width = mixed.shape
    own = jnp.zeros((batch, width), F32)
    for j in range(n_tp):
        columns = slice(j * width, (j + 1) * width)
        fin_send[j] = part[:, columns].astype(BF16)
        own = jnp.where(tp == j, h[:, columns], own)
    copies = exchange("tp", lambda d: fin_send.at[d], lambda k: fin_recv.at[k], fin_sems)
    total = total_of(copies, fin_send[tp].astype(F32), fin_recv)
    mixed[...] = (own + 0.5 * total).astype(BF16)


def dma_sems(n):
    return pltpu.SemaphoreType.DMA((2, n - 1))


def on_device(
    n_kv, n_tp, tokens, first_gain, first_gate, first_up, first_down, mix_gain, w_query,
    key_cache, value_cache, map_weight, head_gain, w_out, second_gain, second_gate, second_up,
    second_down,
):
    batch, own_width = tokens.shape
    depth, hidden = first_gate.shape
    length = key_cache.shape[1]
    columns = w_query.shape[1]
    kv_local = key_cache.shape[2] // HEAD
    group = columns // (kv_local * HEAD)
    pairs = batch // 2
    cw = -(-hidden // (LANES * COL_GROUPS)) * LANES
    vmem = pl.BlockSpec(memory_space=pltpu.VMEM)
    hbm = pl.BlockSpec(memory_space=pl.ANY)
    ffn_buffers = [
        pltpu.VMEM((n_kv, TILE, 2 * cw + LANES), BF16),
        pltpu.VMEM((n_kv - 1, TILE, 2 * cw + LANES), BF16),
        pltpu.VMEM((TILE, cw), BF16),
        pltpu.VMEM((n_kv, TILE, cw), BF16),
    ]
    tp_buffers = [pltpu.VMEM((batch, depth), BF16), pltpu.VMEM((n_tp - 1, batch, depth), BF16)]
    q_tiles = 2 * (batch // TILE) + 1
    return pl.pallas_call(
        functools.partial(
            layer_kernel, n_kv, n_tp, kv_local, group, math.log2(math.e) / math.sqrt(HEAD // MAPS)
        ),
        out_shape=jax.ShapeDtypeStruct((batch, depth // n_tp), BF16),
        in_specs=[vmem] * 6 + [hbm] * 10,
        out_specs=vmem,
        scratch_shapes=[
            pltpu.VMEM(first_gate.shape, BF16),
            pltpu.VMEM(first_up.shape, BF16),
            pltpu.VMEM(first_down.shape, BF16),
            pltpu.VMEM(w_query.shape, BF16),
            pltpu.VMEM((pairs, length, 2 * LANES), BF16),
            pltpu.VMEM((pairs, length, 2 * LANES), BF16),
            pltpu.VMEM(w_out.shape, BF16),
            pltpu.VMEM(second_gate.shape, BF16),
            pltpu.VMEM(second_up.shape, BF16),
            pltpu.VMEM(second_down.shape, BF16),
            pltpu.VMEM((n_tp,) + tokens.shape, BF16),
            *ffn_buffers,
            *tp_buffers,
            pltpu.VMEM((q_tiles, TILE, LANES), BF16),
            pltpu.VMEM((n_kv - 1, q_tiles, TILE, LANES), BF16),
            pltpu.VMEM((pairs, 2 * TILE, 2 * LANES), BF16),
            pltpu.VMEM((n_kv, 2, TILE, LANES), F32),
            pltpu.VMEM((n_kv - 1, 2, TILE, LANES), F32),
            pltpu.VMEM((TILE, LANES), F32),
            pltpu.VMEM((n_kv * TILE, LANES), F32),
            *tp_buffers,
            *ffn_buffers,
            pltpu.VMEM((n_tp, batch, own_width), BF16),
            pltpu.VMEM((n_tp - 1, batch, own_width), BF16),
            pltpu.SemaphoreType.DMA((11 + kv_local * group,)),
            dma_sems(n_tp),
            dma_sems(n_kv),
            dma_sems(n_kv),
            dma_sems(n_tp),
            dma_sems(n_kv),
            dma_sems(n_kv),
            dma_sems(n_kv),
            dma_sems(n_tp),
            dma_sems(n_kv),
            dma_sems(n_kv),
            dma_sems(n_tp),
        ],
        compiler_params=pltpu.CompilerParams(
            collective_id=1, has_side_effects=True, vmem_limit_bytes=VMEM_LIMIT
        ),
    )(
        tokens, first_gain.reshape(1, -1), mix_gain.reshape(1, -1), second_gain.reshape(1, -1),
        map_weight.reshape(1, -1), head_gain.reshape(1, -1),
        first_gate, first_up, first_down, w_query, key_cache, value_cache, w_out,
        second_gate, second_up, second_down,
    )


def solution(mesh):
    placed = (
        P(None, ("kv", "tp")),
        P("kv"),
        P("kv", "tp"),
        P("kv", "tp"),
        P("tp", "kv"),
        P("kv"),
        P("kv", "tp"),
        P(None, "kv", "tp"),
        P(None, "kv", "tp"),
        P("tp"),
        P(),
        P("tp", "kv"),
        P("kv"),
        P("kv", "tp"),
        P("kv", "tp"),
        P("tp", "kv"),
    )
    return jax.shard_map(
        functools.partial(on_device, mesh.shape["kv"], mesh.shape["tp"]),
        mesh=mesh,
        in_specs=placed,
        out_specs=P(None, ("kv", "tp")),
        check_vma=False,
    )
```

```python
import functools
import math

import jax
import jax.numpy as jnp
from jax import lax
from jax.experimental import pallas as pl
from jax.experimental.pallas import tpu as pltpu
from jax.sharding import PartitionSpec as P

HEAD = 64
MAPS = 2
LANES = 128
TILE = 8
EPS = 1e-06
HEAD_SCALE = 0.8
SIDE = 4
ROW_GROUPS = 4
COL_GROUPS = 4
GROUP_ENDS = (5, 10, 14, 16)
F32 = jnp.float32
BF16 = jnp.bfloat16
MESH = pl.DeviceIdType.MESH
VMEM_LIMIT = 60 * 1024 * 1024


def hops(d):
    return min(d, SIDE - d)


def kv_offsets():
    offs = [(a, b) for a in range(SIDE) for b in range(SIDE) if (a, b) != (0, 0)]
    return sorted(offs, key=lambda o: -(hops(o[0]) + hops(o[1])))


def tp_offsets():
    offs = [(a, b) for a in range(SIDE) for b in range(2) if (a, b) != (0, 0)]
    return sorted(offs, key=lambda o: -(2 * hops(o[0]) + o[1]))


def shifted(axis, offset):
    me = lax.axis_index(axis)
    inner = SIDE if axis == "kv" else 2
    high = lax.rem(me // inner + offset[0], SIDE)
    low = lax.rem(lax.rem(me, inner) + offset[1], inner)
    return high * inner + low


OFFSETS = {"kv": kv_offsets(), "tp": tp_offsets()}


def greet():
    barrier = pltpu.get_barrier_semaphore()
    total = 0
    for axis in ("kv", "tp"):
        for offset in OFFSETS[axis]:
            pl.semaphore_signal(
                barrier, inc=1, device_id={axis: shifted(axis, offset)}, device_id_type=MESH
            )
            total += 1
    pl.semaphore_wait(barrier, total)


def exchange(axis, source, target, sems):
    copies = []
    for k, offset in enumerate(OFFSETS[axis]):
        dest = shifted(axis, offset)
        copy = pltpu.make_async_remote_copy(
            src_ref=source(dest),
            dst_ref=target(k),
            send_sem=sems.at[0, k],
            recv_sem=sems.at[1, k],
            device_id={axis: dest},
            device_id_type=MESH,
        )
        copy.start()
        copies.append(copy)
    return copies


def total_of(copies, own, recv):
    total = own
    for k in reversed(range(len(copies))):
        copies[k].wait()
        total = total + recv[k].astype(F32)
    return total


def dot(a, b):
    return jnp.dot(a, b, preferred_element_type=F32)


def row_squares(h):
    return jnp.sum(h * h, axis=1, keepdims=True)


def squares_tile(h):
    s = row_squares(h)
    high = s.astype(BF16).astype(F32)
    lane = lax.broadcasted_iota(jnp.int32, (h.shape[0], LANES), 1)
    return jnp.where(lane < LANES // 2, high, s - high).astype(BF16)


def row_factor(tile, width):
    s = tile[:, :1] + tile[:, LANES // 2 : LANES // 2 + 1]
    return lax.rsqrt(s / width + EPS)


def feed_forward(n_kv, h, gain, w_gate, w_up, w_down, loads, scratch):
    send, recv, act_own, act_all, rs_sems, ag_sems = scratch
    me = lax.axis_index("kv")
    hidden = w_gate.shape[1]
    cw = act_own.shape[1]
    tile = squares_tile(h)
    scaled = (h * gain).astype(BF16)
    loads[0].wait()
    loads[1].wait()
    for c in range(COL_GROUPS):
        low = c * cw
        w = min(cw, hidden - low)
        for base, weight in ((0, w_gate), (cw, w_up)):
            part = dot(scaled, weight[:, low : low + w])
            for r in range(ROW_GROUPS):
                rows = slice(r * TILE, (r + 1) * TILE)
                send[r * COL_GROUPS + c, :, base : base + w] = part[rows].astype(BF16)
                if w < cw:
                    send[r * COL_GROUPS + c, :, base + w : base + cw] = jnp.zeros(
                        (TILE, cw - w), BF16
                    )
        for r in range(ROW_GROUPS):
            send[r * COL_GROUPS + c, :, 2 * cw :] = tile[r * TILE : (r + 1) * TILE]
    copies = exchange("kv", lambda d: send.at[d], lambda k: recv.at[k], rs_sems)
    total = total_of(copies, send[me].astype(F32), recv)
    factor = row_factor(total[:, 2 * cw :], h.shape[1] * n_kv)
    gate = total[:, :cw] * factor
    up = total[:, cw : 2 * cw] * factor
    act = (gate / (1.0 + jnp.exp(-gate)) * up).astype(BF16)
    act_own[...] = act
    act_all[me] = act
    copies = exchange("kv", lambda d: act_own, lambda k: act_all.at[me], ag_sems)
    for copy in copies:
        copy.wait()
    loads[2].wait()
    out = None
    for c in range(COL_GROUPS):
        low = c * cw
        w = min(cw, hidden - low)
        block = jnp.concatenate(
            [act_all[r * COL_GROUPS + c, :, :w].astype(F32) for r in range(ROW_GROUPS)], axis=0
        ).astype(BF16)
        term = dot(block, w_down[low : low + w, :])
        out = term if out is None else out + term
    return out


def sum_over_tp(part, send, recv, sems):
    send[...] = part.astype(BF16)
    copies = exchange("tp", lambda d: send, lambda k: recv.at[k], sems)
    return total_of(copies, send[...].astype(F32), recv)


def query_step(n_kv, h, gain, w_query, q_send, q_recv, q_sems):
    rows = h.shape[0]
    product = dot((h * gain).astype(BF16), w_query[...])
    row = lax.broadcasted_iota(jnp.int32, (rows, LANES), 0)
    lane = lax.broadcasted_iota(jnp.int32, (rows, LANES), 1)
    s = jnp.sum(jnp.where(row == lane, row_squares(h), 0.0), axis=0, keepdims=True)
    high = s.astype(BF16).astype(F32)
    first = lax.broadcasted_iota(jnp.int32, (TILE, LANES), 0)
    stats = jnp.where(first == 0, high, jnp.where(first == 1, s - high, 0.0))
    tiles = rows // TILE
    for r in range(tiles):
        for c in range(2):
            q_send[2 * r + c] = product[
                r * TILE : (r + 1) * TILE, c * LANES : (c + 1) * LANES
            ].astype(BF16)
    q_send[2 * tiles] = stats.astype(BF16)
    copies = exchange("kv", lambda d: q_send, lambda k: q_recv.at[k], q_sems)
    total = total_of(copies, q_send[...].astype(F32), q_recv)
    s = jnp.sum(total[2 * tiles], axis=0, keepdims=True)
    factor = lax.rsqrt(s / (h.shape[1] * n_kv) + EPS)
    factor = jnp.sum(jnp.where(row == lane, factor, 0.0), axis=1, keepdims=True)
    halves = [
        jnp.concatenate([total[2 * r + c] for r in range(tiles)], axis=0) * factor
        for c in range(2)
    ]
    low = lane < HEAD
    first_half = jnp.where(low, halves[0], pltpu.roll(halves[1], HEAD, 1))
    second_half = jnp.where(low, pltpu.roll(halves[0], HEAD, 1), halves[1])
    return first_half.astype(BF16), second_half.astype(BF16)


def spread_queries(q_parts, pairs, qx):
    batch = q_parts[0].shape[0]
    per = qx.shape[1]
    rows = pairs * per
    row = lax.broadcasted_iota(jnp.int32, (rows, batch), 0)
    col = lax.broadcasted_iota(jnp.int32, (rows, batch), 1)
    pick = jnp.where(col == row // per + pairs * lax.rem(row, 2), 1.0, 0.0).astype(BF16)
    wide_row = lax.broadcasted_iota(jnp.int32, (rows, LANES), 0)
    lane = lax.broadcasted_iota(jnp.int32, (rows, LANES), 1)
    which = lax.rem(wide_row // 2, 2)
    y = jnp.where(which == 0, dot(pick, q_parts[0]), dot(pick, q_parts[1]))
    mine = lane // (HEAD // MAPS) == lax.rem(wide_row // 4, 4)
    y = jnp.where(mine, y, 0.0)
    member = lax.rem(wide_row, 2)
    for i in range(2):
        block = jnp.where(member == i, y, 0.0).astype(BF16)
        qx[:, :, i * LANES : (i + 1) * LANES] = block.reshape(pairs, per, LANES)


def scores(qx, k_buf, p):
    return lax.dot_general(qx[p], k_buf[p], (((1,), (1,)), ((), ())), preferred_element_type=F32)


def attention_step(scale, qx, k_buf, v_buf, o_send, o_recv, st_send, st_recv, o_sems, st_sems):
    pairs = qx.shape[0]
    row = lax.broadcasted_iota(jnp.int32, (2 * TILE, LANES), 0)
    lane = lax.broadcasted_iota(jnp.int32, (TILE, LANES), 1)
    first_member = lax.rem(row, 2) == 0
    low = lane < HEAD
    stats = jnp.zeros((TILE, LANES), F32)
    copies = []
    ahead = scores(qx, k_buf, 0)
    begin = 0
    for p in range(pairs):
        s = ahead
        if p + 1 < pairs:
            ahead = scores(qx, k_buf, p + 1)
        peak = jnp.max(s, axis=1, keepdims=True)
        e = jnp.exp2((s - peak) * scale)
        l = jnp.sum(e, axis=1, keepdims=True)
        lse = peak * scale + jnp.log2(l)
        stats = jnp.where(lane == 2 * p, lse[:TILE], stats)
        stats = jnp.where(lane == 2 * p + 1, lse[TILE:], stats)
        o = dot(e.astype(BF16), v_buf[p]) / l
        o = jnp.where(first_member, o[:, :LANES], o[:, LANES:])
        o_send[p] = jnp.where(low, o[:TILE], o[TILE:]).astype(BF16)
        if p + 1 == pairs:
            st_send[...] = stats
        if p + 1 in GROUP_ENDS:
            span = pl.ds(begin, p + 1 - begin)
            sems = o_sems.at[GROUP_ENDS.index(p + 1)]
            copies += exchange(
                "kv", lambda d: o_send.at[span], lambda k: o_recv.at[k, span], sems
            )
            begin = p + 1
    return copies, exchange("kv", lambda d: st_send, lambda k: st_recv.at[k], st_sems)


def selector(sel):
    depth, width = sel.shape
    for j in range(width // LANES):
        row = lax.broadcasted_iota(jnp.int32, (depth, LANES), 0)
        lane = lax.broadcasted_iota(jnp.int32, (depth, LANES), 1)
        count = width // HEAD
        here = (lax.rem(row, count) == 2 * j + lane // HEAD) & (row < 2 * count)
        sel[:, j * LANES : (j + 1) * LANES] = jnp.where(here, 1.0, 0.0).astype(BF16)


def head_weights(map_weight, group, kv_local):
    row = lax.broadcasted_iota(jnp.int32, (TILE, LANES), 0)
    lane = lax.broadcasted_iota(jnp.int32, (TILE, LANES), 1)
    weight = jnp.zeros((TILE, LANES), F32)
    for k in range(kv_local):
        for g in range(group):
            here = (lax.rem(row // 2, group) == g) & (lane // HEAD == k)
            at = k * group + g
            weight = jnp.where(here, map_weight[:, at : at + 1], weight)
    return weight


def merge_heads(copies, st_copies, o_send, o_recv, st_send, st_recv, sel, weight, gain, heads):
    pairs = o_send.shape[0]
    count = 2 * pairs
    others = len(st_copies)
    lane = lax.broadcasted_iota(jnp.int32, (TILE, LANES), 1)
    for copy in st_copies:
        copy.wait()
    lses = [st_send[...]] + [st_recv[k] for k in range(others)]
    peak = functools.reduce(jnp.maximum, lses)
    weights = [jnp.exp2(lse - peak) for lse in lses]
    share = 1.0 / functools.reduce(jnp.add, weights)
    rows = []
    for w in weights:
        w = w * share
        high = w.astype(BF16).astype(F32)
        rest = pltpu.roll(w - high, count, 1)
        rows.append(jnp.where(lane < count, high, jnp.where(lane < 2 * count, rest, 0.0)))
    spread = jnp.concatenate(rows, axis=0).astype(BF16)
    for copy in copies:
        copy.wait()
    low = lane < HEAD
    for j in range(pairs // 2):
        wide = dot(spread, sel[:, 2 * j * LANES : 2 * (j + 1) * LANES])
        for i in range(2):
            p = 2 * j + i
            columns = slice(i * LANES, (i + 1) * LANES)
            outs = [o_send[p].astype(F32)] + [o_recv[k, p].astype(F32) for k in range(others)]
            merged = functools.reduce(
                jnp.add,
                [wide[d * TILE : (d + 1) * TILE, columns] * o for d, o in enumerate(outs)],
            )
            diff = merged - weight * pltpu.roll(merged, TILE // 2, 0)
            square = diff * diff
            left = jnp.sum(jnp.where(low, square, 0.0), axis=1, keepdims=True)
            right = jnp.sum(jnp.where(low, 0.0, square), axis=1, keepdims=True)
            mean = jnp.where(low, left, right) / HEAD
            heads[p * TILE : (p + 1) * TILE, :] = diff * lax.rsqrt(mean + EPS) * gain


def start_loads(pairs, sems):
    loads = [pltpu.make_async_copy(a, b, sems.at[i]) for i, (a, b) in enumerate(pairs)]
    for load in loads:
        load.start()
    return loads


def layer_kernel(
    n_kv, n_tp, kv_local, group, scale,
    tokens_any, gain1_any, gain_mix_any, gain2_any, weight_any, head_gain_any,
    gate1_any, up1_any, down1_any, query_any, key_any, value_any, out_any,
    gate2_any, up2_any, down2_any,
    mixed,
    tokens, first_gain, mix_gain, second_gain, map_weight, head_gain,
    w_gate1, w_up1, w_down1, w_query, k_buf, v_buf, w_out, w_gate2, w_up2, w_down2,
    tok_all, rs1_send, rs1_recv, act1_own, act1_all, tp1_send, tp1_recv, q_send, q_recv, qx,
    o_send, o_recv, st_send, st_recv, sel, head_all, tp2_send, tp2_recv,
    rs2_send, rs2_recv, act2_own, act2_all, fin_send, fin_recv,
    small_sems, load_sems, tok_sems, rs1_sems, ag1_sems, tp1_sems, q_sems, o_sems, st_sems,
    tp2_sems, rs2_sems, ag2_sems, fin_sems,
):
    pairs = k_buf.shape[0]
    small = start_loads(
        (
            (tokens_any, tokens),
            (gain1_any, first_gain),
            (gain_mix_any, mix_gain),
            (gain2_any, second_gain),
            (weight_any, map_weight),
            (head_gain_any, head_gain),
        ),
        small_sems,
    )
    loads = start_loads(
        (
            (gate1_any, w_gate1),
            (up1_any, w_up1),
            (down1_any, w_down1),
            (query_any, w_query),
            (key_any.at[:pairs], k_buf.at[:, :, :LANES]),
            (key_any.at[pairs:], k_buf.at[:, :, LANES:]),
            (value_any.at[:pairs], v_buf.at[:, :, :LANES]),
            (value_any.at[pairs:], v_buf.at[:, :, LANES:]),
            (gate2_any, w_gate2),
            (up2_any, w_up2),
            (down2_any, w_down2),
        )
        + tuple(
            (
                out_any.at[pl.ds((k * group + g) * HEAD, HEAD)],
                w_out.at[pl.ds((g * kv_local + k) * HEAD, HEAD)],
            )
            for k in range(kv_local)
            for g in range(group)
        ),
        load_sems,
    )
    greet()
    for load in small:
        load.wait()
    tp = lax.axis_index("tp")
    tok_all[tp] = tokens[...]
    copies = exchange("tp", lambda d: tokens, lambda k: tok_all.at[tp], tok_sems)
    selector(sel)
    for copy in copies:
        copy.wait()
    h = jnp.concatenate([tok_all[j].astype(F32) for j in range(n_tp)], axis=1)
    part = feed_forward(
        n_kv, h, first_gain[...], w_gate1, w_up1, w_down1, loads[:3],
        (rs1_send, rs1_recv, act1_own, act1_all, rs1_sems, ag1_sems),
    )
    h = h + 0.5 * sum_over_tp(part, tp1_send, tp1_recv, tp1_sems)
    loads[3].wait()
    q_parts = query_step(n_kv, h, mix_gain[...], w_query, q_send, q_recv, q_sems)
    spread_queries(q_parts, pairs, qx)
    for load in loads[4:8]:
        load.wait()
    copies, st_copies = attention_step(
        scale, qx, k_buf, v_buf, o_send, o_recv, st_send, st_recv, o_sems, st_sems
    )
    weight = head_weights(map_weight, group, kv_local)
    gain = jnp.concatenate([head_gain[...] * HEAD_SCALE] * kv_local, axis=1)
    merge_heads(
        copies, st_copies, o_send, o_recv, st_send, st_recv, sel, weight, gain, head_all
    )
    heads = jnp.concatenate(
        [
            jnp.concatenate(
                [head_all[pl.ds(2 * g + i, pairs, stride=TILE), :] for g in range(group)], axis=1
            )
            for i in range(2)
        ],
        axis=0,
    ).astype(BF16)
    for load in loads[11:]:
        load.wait()
    h = h + sum_over_tp(dot(heads, w_out[...]), tp2_send, tp2_recv, tp2_sems)
    part = feed_forward(
        n_kv, h, second_gain[...], w_gate2, w_up2, w_down2, loads[8:11],
        (rs2_send, rs2_recv, act2_own, act2_all, rs2_sems, ag2_sems),
    )
    batch, width = mixed.shape
    own = jnp.zeros((batch, width), F32)
    for j in range(n_tp):
        columns = slice(j * width, (j + 1) * width)
        fin_send[j] = part[:, columns].astype(BF16)
        own = jnp.where(tp == j, h[:, columns], own)
    copies = exchange("tp", lambda d: fin_send.at[d], lambda k: fin_recv.at[k], fin_sems)
    total = total_of(copies, fin_send[tp].astype(F32), fin_recv)
    mixed[...] = (own + 0.5 * total).astype(BF16)


def dma_sems(n):
    return pltpu.SemaphoreType.DMA((2, n - 1))


def on_device(
    n_kv, n_tp, tokens, first_gain, first_gate, first_up, first_down, mix_gain, w_query,
    key_cache, value_cache, map_weight, head_gain, w_out, second_gain, second_gate, second_up,
    second_down,
):
    batch, own_width = tokens.shape
    depth, hidden = first_gate.shape
    length = key_cache.shape[1]
    columns = w_query.shape[1]
    kv_local = key_cache.shape[2] // HEAD
    group = columns // (kv_local * HEAD)
    pairs = batch // 2
    cw = -(-hidden // (LANES * COL_GROUPS)) * LANES
    hbm = pl.BlockSpec(memory_space=pl.ANY)
    ffn_buffers = [
        pltpu.VMEM((n_kv, TILE, 2 * cw + LANES), BF16),
        pltpu.VMEM((n_kv - 1, TILE, 2 * cw + LANES), BF16),
        pltpu.VMEM((TILE, cw), BF16),
        pltpu.VMEM((n_kv, TILE, cw), BF16),
    ]
    tp_buffers = [pltpu.VMEM((batch, depth), BF16), pltpu.VMEM((n_tp - 1, batch, depth), BF16)]
    q_tiles = 2 * (batch // TILE) + 1
    return pl.pallas_call(
        functools.partial(
            layer_kernel, n_kv, n_tp, kv_local, group, math.log2(math.e) / math.sqrt(HEAD // MAPS)
        ),
        out_shape=pltpu.VMEM((batch, depth // n_tp), BF16),
        in_specs=[hbm] * 16,
        out_specs=pl.BlockSpec(memory_space=pltpu.VMEM),
        scratch_shapes=[
            pltpu.VMEM(tokens.shape, BF16),
            pltpu.VMEM((1, depth), F32),
            pltpu.VMEM((1, depth), F32),
            pltpu.VMEM((1, depth), F32),
            pltpu.VMEM((1, kv_local * group), F32),
            pltpu.VMEM((1, HEAD), F32),
            pltpu.VMEM(first_gate.shape, BF16),
            pltpu.VMEM(first_up.shape, BF16),
            pltpu.VMEM(first_down.shape, BF16),
            pltpu.VMEM(w_query.shape, BF16),
            pltpu.VMEM((pairs, length, 2 * LANES), BF16),
            pltpu.VMEM((pairs, length, 2 * LANES), BF16),
            pltpu.VMEM(w_out.shape, BF16),
            pltpu.VMEM(second_gate.shape, BF16),
            pltpu.VMEM(second_up.shape, BF16),
            pltpu.VMEM(second_down.shape, BF16),
            pltpu.VMEM((n_tp,) + tokens.shape, BF16),
            *ffn_buffers,
            *tp_buffers,
            pltpu.VMEM((q_tiles, TILE, LANES), BF16),
            pltpu.VMEM((n_kv - 1, q_tiles, TILE, LANES), BF16),
            pltpu.VMEM((pairs, 2 * TILE, 2 * LANES), BF16),
            pltpu.VMEM((pairs, TILE, LANES), BF16),
            pltpu.VMEM((n_kv - 1, pairs, TILE, LANES), BF16),
            pltpu.VMEM((TILE, LANES), F32),
            pltpu.VMEM((n_kv - 1, TILE, LANES), F32),
            pltpu.VMEM((LANES, pairs * LANES), BF16),
            pltpu.VMEM((pairs * TILE, LANES), F32),
            *tp_buffers,
            *ffn_buffers,
            pltpu.VMEM((n_tp, batch, own_width), BF16),
            pltpu.VMEM((n_tp - 1, batch, own_width), BF16),
            pltpu.SemaphoreType.DMA((6,)),
            pltpu.SemaphoreType.DMA((11 + kv_local * group,)),
            dma_sems(n_tp),
            dma_sems(n_kv),
            dma_sems(n_kv),
            dma_sems(n_tp),
            dma_sems(n_kv),
            pltpu.SemaphoreType.DMA((len(GROUP_ENDS), 2, n_kv - 1)),
            dma_sems(n_kv),
            dma_sems(n_tp),
            dma_sems(n_kv),
            dma_sems(n_kv),
            dma_sems(n_tp),
        ],
        compiler_params=pltpu.CompilerParams(
            collective_id=1, has_side_effects=True, vmem_limit_bytes=VMEM_LIMIT
        ),
    )(
        tokens, first_gain.reshape(1, -1), mix_gain.reshape(1, -1), second_gain.reshape(1, -1),
        map_weight.reshape(1, -1), head_gain.reshape(1, -1),
        first_gate, first_up, first_down, w_query, key_cache, value_cache, w_out,
        second_gate, second_up, second_down,
    )


def solution(mesh):
    placed = (
        P(None, ("kv", "tp")),
        P("kv"),
        P("kv", "tp"),
        P("kv", "tp"),
        P("tp", "kv"),
        P("kv"),
        P("kv", "tp"),
        P(None, "kv", "tp"),
        P(None, "kv", "tp"),
        P("tp"),
        P(),
        P("tp", "kv"),
        P("kv"),
        P("kv", "tp"),
        P("kv", "tp"),
        P("tp", "kv"),
    )
    return jax.shard_map(
        functools.partial(on_device, mesh.shape["kv"], mesh.shape["tp"]),
        mesh=mesh,
        in_specs=placed,
        out_specs=P(None, ("kv", "tp")),
        check_vma=False,
    )
```

```python
import functools
import math

import jax
import jax.numpy as jnp
from jax import lax
from jax.experimental import pallas as pl
from jax.experimental.pallas import tpu as pltpu
from jax.sharding import PartitionSpec as P

HEAD = 64
MAPS = 2
LANES = 128
TILE = 8
EPS = 1e-06
HEAD_SCALE = 0.8
SIDE = 4
ROW_GROUPS = 4
COL_GROUPS = 4
GROUP_ENDS = (5, 10, 14, 16)
F32 = jnp.float32
BF16 = jnp.bfloat16
MESH = pl.DeviceIdType.MESH
VMEM_LIMIT = 60 * 1024 * 1024


def hops(d):
    return min(d, SIDE - d)


def kv_offsets():
    offs = [(a, b) for a in range(SIDE) for b in range(SIDE) if (a, b) != (0, 0)]
    return sorted(offs, key=lambda o: -(hops(o[0]) + hops(o[1])))


def tp_offsets():
    offs = [(a, b) for a in range(SIDE) for b in range(2) if (a, b) != (0, 0)]
    return sorted(offs, key=lambda o: -(2 * hops(o[0]) + o[1]))


def shifted(axis, offset):
    me = lax.axis_index(axis)
    inner = SIDE if axis == "kv" else 2
    high = lax.rem(me // inner + offset[0], SIDE)
    low = lax.rem(lax.rem(me, inner) + offset[1], inner)
    return high * inner + low


OFFSETS = {"kv": kv_offsets(), "tp": tp_offsets()}


def greet():
    barrier = pltpu.get_barrier_semaphore()
    total = 0
    for axis in ("kv", "tp"):
        for offset in OFFSETS[axis]:
            pl.semaphore_signal(
                barrier, inc=1, device_id={axis: shifted(axis, offset)}, device_id_type=MESH
            )
            total += 1
    pl.semaphore_wait(barrier, total)


def exchange(axis, source, target, sems):
    copies = []
    for k, offset in enumerate(OFFSETS[axis]):
        dest = shifted(axis, offset)
        copy = pltpu.make_async_remote_copy(
            src_ref=source(dest),
            dst_ref=target(k),
            send_sem=sems.at[0, k],
            recv_sem=sems.at[1, k],
            device_id={axis: dest},
            device_id_type=MESH,
        )
        copy.start()
        copies.append(copy)
    return copies


def total_of(copies, own, recv):
    total = own
    for k in reversed(range(len(copies))):
        copies[k].wait()
        total = total + recv[k].astype(F32)
    return total


def dot(a, b):
    return jnp.dot(a, b, preferred_element_type=F32)


def row_squares(h):
    return jnp.sum(h * h, axis=1, keepdims=True)


def squares_tile(h):
    s = row_squares(h)
    high = s.astype(BF16).astype(F32)
    lane = lax.broadcasted_iota(jnp.int32, (h.shape[0], LANES), 1)
    return jnp.where(lane < LANES // 2, high, s - high).astype(BF16)


def row_factor(tile, width):
    s = tile[:, :1] + tile[:, LANES // 2 : LANES // 2 + 1]
    return lax.rsqrt(s / width + EPS)


def feed_forward(n_kv, h, gain, w_gate, w_up, w_down, loads, scratch):
    send, recv, act_own, act_all, rs_sems, ag_sems = scratch
    me = lax.axis_index("kv")
    hidden = w_gate.shape[1]
    cw = act_own.shape[1]
    tile = squares_tile(h)
    scaled = (h * gain).astype(BF16)
    loads[0].wait()
    loads[1].wait()
    for c in range(COL_GROUPS):
        low = c * cw
        w = min(cw, hidden - low)
        for base, weight in ((0, w_gate), (cw, w_up)):
            part = dot(scaled, weight[:, low : low + w])
            for r in range(ROW_GROUPS):
                rows = slice(r * TILE, (r + 1) * TILE)
                send[r * COL_GROUPS + c, :, base : base + w] = part[rows].astype(BF16)
                if w < cw:
                    send[r * COL_GROUPS + c, :, base + w : base + cw] = jnp.zeros(
                        (TILE, cw - w), BF16
                    )
        for r in range(ROW_GROUPS):
            send[r * COL_GROUPS + c, :, 2 * cw :] = tile[r * TILE : (r + 1) * TILE]
    copies = exchange("kv", lambda d: send.at[d], lambda k: recv.at[k], rs_sems)
    total = total_of(copies, send[me].astype(F32), recv)
    factor = row_factor(total[:, 2 * cw :], h.shape[1] * n_kv)
    gate = total[:, :cw] * factor
    up = total[:, cw : 2 * cw] * factor
    act = (gate / (1.0 + jnp.exp(-gate)) * up).astype(BF16)
    act_own[...] = act
    act_all[me] = act
    copies = exchange("kv", lambda d: act_own, lambda k: act_all.at[me], ag_sems)
    for copy in copies:
        copy.wait()
    loads[2].wait()
    out = None
    for c in range(COL_GROUPS):
        low = c * cw
        w = min(cw, hidden - low)
        block = jnp.concatenate(
            [act_all[r * COL_GROUPS + c, :, :w].astype(F32) for r in range(ROW_GROUPS)], axis=0
        ).astype(BF16)
        term = dot(block, w_down[low : low + w, :])
        out = term if out is None else out + term
    return out


def sum_over_tp(part, send, recv, sems):
    send[...] = part.astype(BF16)
    copies = exchange("tp", lambda d: send, lambda k: recv.at[k], sems)
    return total_of(copies, send[...].astype(F32), recv)


def query_step(n_kv, h, gain, w_query, q_send, q_recv, q_sems):
    rows = h.shape[0]
    product = dot((h * gain).astype(BF16), w_query[...])
    row = lax.broadcasted_iota(jnp.int32, (rows, LANES), 0)
    lane = lax.broadcasted_iota(jnp.int32, (rows, LANES), 1)
    s = jnp.sum(jnp.where(row == lane, row_squares(h), 0.0), axis=0, keepdims=True)
    high = s.astype(BF16).astype(F32)
    first = lax.broadcasted_iota(jnp.int32, (TILE, LANES), 0)
    stats = jnp.where(first == 0, high, jnp.where(first == 1, s - high, 0.0))
    tiles = rows // TILE
    for r in range(tiles):
        for c in range(2):
            q_send[2 * r + c] = product[
                r * TILE : (r + 1) * TILE, c * LANES : (c + 1) * LANES
            ].astype(BF16)
    q_send[2 * tiles] = stats.astype(BF16)
    copies = exchange("kv", lambda d: q_send, lambda k: q_recv.at[k], q_sems)
    total = total_of(copies, q_send[...].astype(F32), q_recv)
    s = jnp.sum(total[2 * tiles], axis=0, keepdims=True)
    factor = lax.rsqrt(s / (h.shape[1] * n_kv) + EPS)
    factor = jnp.sum(jnp.where(row == lane, factor, 0.0), axis=1, keepdims=True)
    halves = [
        jnp.concatenate([total[2 * r + c] for r in range(tiles)], axis=0) * factor
        for c in range(2)
    ]
    low = lane < HEAD
    first_half = jnp.where(low, halves[0], pltpu.roll(halves[1], HEAD, 1))
    second_half = jnp.where(low, pltpu.roll(halves[0], HEAD, 1), halves[1])
    return first_half.astype(BF16), second_half.astype(BF16)


def spread_queries(q_parts, pairs, qx):
    batch = q_parts[0].shape[0]
    per = qx.shape[1]
    rows = pairs * per
    row = lax.broadcasted_iota(jnp.int32, (rows, batch), 0)
    col = lax.broadcasted_iota(jnp.int32, (rows, batch), 1)
    pick = jnp.where(col == row // per + pairs * lax.rem(row, 2), 1.0, 0.0).astype(BF16)
    wide_row = lax.broadcasted_iota(jnp.int32, (rows, LANES), 0)
    lane = lax.broadcasted_iota(jnp.int32, (rows, LANES), 1)
    which = lax.rem(wide_row // 2, 2)
    y = jnp.where(which == 0, dot(pick, q_parts[0]), dot(pick, q_parts[1]))
    mine = lane // (HEAD // MAPS) == lax.rem(wide_row // 4, 4)
    y = jnp.where(mine, y, 0.0)
    member = lax.rem(wide_row, 2)
    for i in range(2):
        block = jnp.where(member == i, y, 0.0).astype(BF16)
        qx[:, :, i * LANES : (i + 1) * LANES] = block.reshape(pairs, per, LANES)


def scores(qx, k_buf, p):
    return lax.dot_general(qx[p], k_buf[p], (((1,), (1,)), ((), ())), preferred_element_type=F32)


def attention_step(scale, qx, k_buf, v_buf, o_send, o_recv, st_send, st_recv, o_sems, st_sems):
    pairs = qx.shape[0]
    row = lax.broadcasted_iota(jnp.int32, (2 * TILE, LANES), 0)
    lane = lax.broadcasted_iota(jnp.int32, (TILE, LANES), 1)
    first_member = lax.rem(row, 2) == 0
    low = lane < HEAD
    stats = jnp.zeros((TILE, LANES), F32)
    copies = []
    ahead = scores(qx, k_buf, 0)
    begin = 0
    for p in range(pairs):
        s = ahead
        if p + 1 < pairs:
            ahead = scores(qx, k_buf, p + 1)
        peak = jnp.max(s, axis=1, keepdims=True)
        e = jnp.exp2((s - peak) * scale)
        l = jnp.sum(e, axis=1, keepdims=True)
        lse = peak * scale + jnp.log2(l)
        stats = jnp.where(lane == 2 * p, lse[:TILE], stats)
        stats = jnp.where(lane == 2 * p + 1, lse[TILE:], stats)
        o = dot(e.astype(BF16), v_buf[p]) / l
        o = jnp.where(first_member, o[:, :LANES], o[:, LANES:])
        o_send[p] = jnp.where(low, o[:TILE], o[TILE:]).astype(BF16)
        if p + 1 == pairs:
            st_send[...] = stats
        if p + 1 in GROUP_ENDS:
            span = pl.ds(begin, p + 1 - begin)
            sems = o_sems.at[GROUP_ENDS.index(p + 1)]
            copies += exchange(
                "kv", lambda d: o_send.at[span], lambda k: o_recv.at[k, span], sems
            )
            begin = p + 1
    return copies, exchange("kv", lambda d: st_send, lambda k: st_recv.at[k], st_sems)


def selector(sel):
    depth, width = sel.shape
    for j in range(width // LANES):
        row = lax.broadcasted_iota(jnp.int32, (depth, LANES), 0)
        lane = lax.broadcasted_iota(jnp.int32, (depth, LANES), 1)
        count = width // HEAD
        here = (lax.rem(row, count) == 2 * j + lane // HEAD) & (row < 2 * count)
        sel[:, j * LANES : (j + 1) * LANES] = jnp.where(here, 1.0, 0.0).astype(BF16)


def head_weights(map_weight, group, kv_local):
    row = lax.broadcasted_iota(jnp.int32, (TILE, LANES), 0)
    lane = lax.broadcasted_iota(jnp.int32, (TILE, LANES), 1)
    weight = jnp.zeros((TILE, LANES), F32)
    for k in range(kv_local):
        for g in range(group):
            here = (lax.rem(row // 2, group) == g) & (lane // HEAD == k)
            at = k * group + g
            weight = jnp.where(here, map_weight[:, at : at + 1], weight)
    return weight


def merge_heads(copies, st_copies, o_send, o_recv, st_send, st_recv, sel, weight, gain, heads):
    pairs = o_send.shape[0]
    count = 2 * pairs
    others = len(st_copies)
    lane = lax.broadcasted_iota(jnp.int32, (TILE, LANES), 1)
    for copy in st_copies:
        copy.wait()
    lses = [st_send[...]] + [st_recv[k] for k in range(others)]
    peak = functools.reduce(jnp.maximum, lses)
    weights = [jnp.exp2(lse - peak) for lse in lses]
    share = 1.0 / functools.reduce(jnp.add, weights)
    rows = []
    for w in weights:
        w = w * share
        high = w.astype(BF16).astype(F32)
        rest = pltpu.roll(w - high, count, 1)
        rows.append(jnp.where(lane < count, high, jnp.where(lane < 2 * count, rest, 0.0)))
    spread = jnp.concatenate(rows, axis=0).astype(BF16)
    for copy in copies:
        copy.wait()
    low = lane < HEAD
    for j in range(pairs // 2):
        wide = dot(spread, sel[:, 2 * j * LANES : 2 * (j + 1) * LANES])
        for i in range(2):
            p = 2 * j + i
            columns = slice(i * LANES, (i + 1) * LANES)
            outs = [o_send[p].astype(F32)] + [o_recv[k, p].astype(F32) for k in range(others)]
            merged = functools.reduce(
                jnp.add,
                [wide[d * TILE : (d + 1) * TILE, columns] * o for d, o in enumerate(outs)],
            )
            diff = merged - weight * pltpu.roll(merged, TILE // 2, 0)
            square = diff * diff
            left = jnp.sum(jnp.where(low, square, 0.0), axis=1, keepdims=True)
            right = jnp.sum(jnp.where(low, 0.0, square), axis=1, keepdims=True)
            mean = jnp.where(low, left, right) / HEAD
            heads[p * TILE : (p + 1) * TILE, :] = diff * lax.rsqrt(mean + EPS) * gain


def start_loads(pairs, sems):
    loads = [pltpu.make_async_copy(a, b, sems.at[i]) for i, (a, b) in enumerate(pairs)]
    for load in loads:
        load.start()
    return loads


def layer_kernel(
    n_kv, n_tp, kv_local, group, scale,
    tokens_any, gain1_any, gain_mix_any, gain2_any, weight_any, head_gain_any,
    gate1_any, up1_any, down1_any, query_any, key_any, value_any, out_any,
    gate2_any, up2_any, down2_any,
    mixed,
    tokens, first_gain, mix_gain, second_gain, map_weight, head_gain,
    w_gate1, w_up1, w_down1, w_query, k_buf, v_buf, w_out, w_gate2, w_up2, w_down2,
    tok_all, rs1_send, rs1_recv, act1_own, act1_all, tp1_send, tp1_recv, q_send, q_recv, qx,
    o_send, o_recv, st_send, st_recv, sel, head_all, tp2_send, tp2_recv,
    rs2_send, rs2_recv, act2_own, act2_all, fin_send, fin_recv,
    small_sems, load_sems, cache_sems, tok_sems, rs1_sems, ag1_sems, tp1_sems, q_sems, o_sems, st_sems,
    tp2_sems, rs2_sems, ag2_sems, fin_sems,
):
    pairs = k_buf.shape[0]
    small = start_loads(
        (
            (tokens_any, tokens),
            (gain1_any, first_gain),
            (gain_mix_any, mix_gain),
            (gain2_any, second_gain),
            (weight_any, map_weight),
            (head_gain_any, head_gain),
        ),
        small_sems,
    )
    loads = start_loads(
        (
            (gate1_any, w_gate1),
            (up1_any, w_up1),
            (down1_any, w_down1),
            (query_any, w_query),
            (gate2_any, w_gate2),
            (up2_any, w_up2),
            (down2_any, w_down2),
        )
        + tuple(
            (
                out_any.at[pl.ds((k * group + g) * HEAD, HEAD)],
                w_out.at[pl.ds((g * kv_local + k) * HEAD, HEAD)],
            )
            for k in range(kv_local)
            for g in range(group)
        ),
        load_sems,
    )
    greet()
    cache_loads = start_loads(
        (
            (key_any.at[:pairs], k_buf.at[:, :, :LANES]),
            (key_any.at[pairs:], k_buf.at[:, :, LANES:]),
            (value_any.at[:pairs], v_buf.at[:, :, :LANES]),
            (value_any.at[pairs:], v_buf.at[:, :, LANES:]),
        ),
        cache_sems,
    )
    for load in small:
        load.wait()
    tp = lax.axis_index("tp")
    tok_all[tp] = tokens[...]
    copies = exchange("tp", lambda d: tokens, lambda k: tok_all.at[tp], tok_sems)
    selector(sel)
    for copy in copies:
        copy.wait()
    h = jnp.concatenate([tok_all[j].astype(F32) for j in range(n_tp)], axis=1)
    part = feed_forward(
        n_kv, h, first_gain[...], w_gate1, w_up1, w_down1, loads[:3],
        (rs1_send, rs1_recv, act1_own, act1_all, rs1_sems, ag1_sems),
    )
    h = h + 0.5 * sum_over_tp(part, tp1_send, tp1_recv, tp1_sems)
    loads[3].wait()
    q_parts = query_step(n_kv, h, mix_gain[...], w_query, q_send, q_recv, q_sems)
    spread_queries(q_parts, pairs, qx)
    for load in cache_loads:
        load.wait()
    copies, st_copies = attention_step(
        scale, qx, k_buf, v_buf, o_send, o_recv, st_send, st_recv, o_sems, st_sems
    )
    weight = head_weights(map_weight, group, kv_local)
    gain = jnp.concatenate([head_gain[...] * HEAD_SCALE] * kv_local, axis=1)
    merge_heads(
        copies, st_copies, o_send, o_recv, st_send, st_recv, sel, weight, gain, head_all
    )
    heads = jnp.concatenate(
        [
            jnp.concatenate(
                [head_all[pl.ds(2 * g + i, pairs, stride=TILE), :] for g in range(group)], axis=1
            )
            for i in range(2)
        ],
        axis=0,
    ).astype(BF16)
    for load in loads[7:]:
        load.wait()
    h = h + sum_over_tp(dot(heads, w_out[...]), tp2_send, tp2_recv, tp2_sems)
    part = feed_forward(
        n_kv, h, second_gain[...], w_gate2, w_up2, w_down2, loads[4:7],
        (rs2_send, rs2_recv, act2_own, act2_all, rs2_sems, ag2_sems),
    )
    batch, width = mixed.shape
    own = jnp.zeros((batch, width), F32)
    for j in range(n_tp):
        columns = slice(j * width, (j + 1) * width)
        fin_send[j] = part[:, columns].astype(BF16)
        own = jnp.where(tp == j, h[:, columns], own)
    copies = exchange("tp", lambda d: fin_send.at[d], lambda k: fin_recv.at[k], fin_sems)
    total = total_of(copies, fin_send[tp].astype(F32), fin_recv)
    mixed[...] = (own + 0.5 * total).astype(BF16)


def dma_sems(n):
    return pltpu.SemaphoreType.DMA((2, n - 1))


def on_device(
    n_kv, n_tp, tokens, first_gain, first_gate, first_up, first_down, mix_gain, w_query,
    key_cache, value_cache, map_weight, head_gain, w_out, second_gain, second_gate, second_up,
    second_down,
):
    batch, own_width = tokens.shape
    depth, hidden = first_gate.shape
    length = key_cache.shape[1]
    columns = w_query.shape[1]
    kv_local = key_cache.shape[2] // HEAD
    group = columns // (kv_local * HEAD)
    pairs = batch // 2
    cw = -(-hidden // (LANES * COL_GROUPS)) * LANES
    hbm = pl.BlockSpec(memory_space=pl.ANY)
    ffn_buffers = [
        pltpu.VMEM((n_kv, TILE, 2 * cw + LANES), BF16),
        pltpu.VMEM((n_kv - 1, TILE, 2 * cw + LANES), BF16),
        pltpu.VMEM((TILE, cw), BF16),
        pltpu.VMEM((n_kv, TILE, cw), BF16),
    ]
    tp_buffers = [pltpu.VMEM((batch, depth), BF16), pltpu.VMEM((n_tp - 1, batch, depth), BF16)]
    q_tiles = 2 * (batch // TILE) + 1
    return pl.pallas_call(
        functools.partial(
            layer_kernel, n_kv, n_tp, kv_local, group, math.log2(math.e) / math.sqrt(HEAD // MAPS)
        ),
        out_shape=pltpu.VMEM((batch, depth // n_tp), BF16),
        in_specs=[hbm] * 16,
        out_specs=pl.BlockSpec(memory_space=pltpu.VMEM),
        scratch_shapes=[
            pltpu.VMEM(tokens.shape, BF16),
            pltpu.VMEM((1, depth), F32),
            pltpu.VMEM((1, depth), F32),
            pltpu.VMEM((1, depth), F32),
            pltpu.VMEM((1, kv_local * group), F32),
            pltpu.VMEM((1, HEAD), F32),
            pltpu.VMEM(first_gate.shape, BF16),
            pltpu.VMEM(first_up.shape, BF16),
            pltpu.VMEM(first_down.shape, BF16),
            pltpu.VMEM(w_query.shape, BF16),
            pltpu.VMEM((pairs, length, 2 * LANES), BF16),
            pltpu.VMEM((pairs, length, 2 * LANES), BF16),
            pltpu.VMEM(w_out.shape, BF16),
            pltpu.VMEM(second_gate.shape, BF16),
            pltpu.VMEM(second_up.shape, BF16),
            pltpu.VMEM(second_down.shape, BF16),
            pltpu.VMEM((n_tp,) + tokens.shape, BF16),
            *ffn_buffers,
            *tp_buffers,
            pltpu.VMEM((q_tiles, TILE, LANES), BF16),
            pltpu.VMEM((n_kv - 1, q_tiles, TILE, LANES), BF16),
            pltpu.VMEM((pairs, 2 * TILE, 2 * LANES), BF16),
            pltpu.VMEM((pairs, TILE, LANES), BF16),
            pltpu.VMEM((n_kv - 1, pairs, TILE, LANES), BF16),
            pltpu.VMEM((TILE, LANES), F32),
            pltpu.VMEM((n_kv - 1, TILE, LANES), F32),
            pltpu.VMEM((LANES, pairs * LANES), BF16),
            pltpu.VMEM((pairs * TILE, LANES), F32),
            *tp_buffers,
            *ffn_buffers,
            pltpu.VMEM((n_tp, batch, own_width), BF16),
            pltpu.VMEM((n_tp - 1, batch, own_width), BF16),
            pltpu.SemaphoreType.DMA((6,)),
            pltpu.SemaphoreType.DMA((7 + kv_local * group,)),
            pltpu.SemaphoreType.DMA((4,)),
            dma_sems(n_tp),
            dma_sems(n_kv),
            dma_sems(n_kv),
            dma_sems(n_tp),
            dma_sems(n_kv),
            pltpu.SemaphoreType.DMA((len(GROUP_ENDS), 2, n_kv - 1)),
            dma_sems(n_kv),
            dma_sems(n_tp),
            dma_sems(n_kv),
            dma_sems(n_kv),
            dma_sems(n_tp),
        ],
        compiler_params=pltpu.CompilerParams(
            collective_id=1, has_side_effects=True, vmem_limit_bytes=VMEM_LIMIT
        ),
    )(
        tokens, first_gain.reshape(1, -1), mix_gain.reshape(1, -1), second_gain.reshape(1, -1),
        map_weight.reshape(1, -1), head_gain.reshape(1, -1),
        first_gate, first_up, first_down, w_query, key_cache, value_cache, w_out,
        second_gate, second_up, second_down,
    )


def solution(mesh):
    placed = (
        P(None, ("kv", "tp")),
        P("kv"),
        P("kv", "tp"),
        P("kv", "tp"),
        P("tp", "kv"),
        P("kv"),
        P("kv", "tp"),
        P(None, "kv", "tp"),
        P(None, "kv", "tp"),
        P("tp"),
        P(),
        P("tp", "kv"),
        P("kv"),
        P("kv", "tp"),
        P("kv", "tp"),
        P("tp", "kv"),
    )
    return jax.shard_map(
        functools.partial(on_device, mesh.shape["kv"], mesh.shape["tp"]),
        mesh=mesh,
        in_specs=placed,
        out_specs=P(None, ("kv", "tp")),
        check_vma=False,
    )
```

```python
import functools
import math

import jax
import jax.numpy as jnp
from jax import lax
from jax.experimental import pallas as pl
from jax.experimental.pallas import tpu as pltpu
from jax.sharding import PartitionSpec as P

HEAD = 64
MAPS = 2
LANES = 128
TILE = 8
EPS = 1e-06
HEAD_SCALE = 0.8
SIDE = 4
ROW_GROUPS = 4
COL_GROUPS = 4
GROUP_ENDS = (8, 16)
F32 = jnp.float32
BF16 = jnp.bfloat16
MESH = pl.DeviceIdType.MESH
VMEM_LIMIT = 60 * 1024 * 1024


def hops(d):
    return min(d, SIDE - d)


def kv_offsets():
    offs = [(a, b) for a in range(SIDE) for b in range(SIDE) if (a, b) != (0, 0)]
    return sorted(offs, key=lambda o: -(hops(o[0]) + hops(o[1])))


def tp_offsets():
    offs = [(a, b) for a in range(SIDE) for b in range(2) if (a, b) != (0, 0)]
    return sorted(offs, key=lambda o: -(2 * hops(o[0]) + o[1]))


def shifted(axis, offset):
    me = lax.axis_index(axis)
    inner = SIDE if axis == "kv" else 2
    high = lax.rem(me // inner + offset[0], SIDE)
    low = lax.rem(lax.rem(me, inner) + offset[1], inner)
    return high * inner + low


OFFSETS = {"kv": kv_offsets(), "tp": tp_offsets()}


def greet():
    barrier = pltpu.get_barrier_semaphore()
    total = 0
    for axis in ("kv", "tp"):
        for offset in OFFSETS[axis]:
            pl.semaphore_signal(
                barrier, inc=1, device_id={axis: shifted(axis, offset)}, device_id_type=MESH
            )
            total += 1
    pl.semaphore_wait(barrier, total)


def exchange(axis, source, target, send_sem, recv_sem):
    copies = []
    for k, offset in enumerate(OFFSETS[axis]):
        dest = shifted(axis, offset)
        copy = pltpu.make_async_remote_copy(
            src_ref=source(dest),
            dst_ref=target(k),
            send_sem=send_sem,
            recv_sem=recv_sem(k),
            device_id={axis: dest},
            device_id_type=MESH,
        )
        copy.start()
        copies.append(copy)
    return copies


def drain(axis, ref, sem):
    peer = shifted(axis, OFFSETS[axis][0])
    pltpu.make_async_remote_copy(
        src_ref=ref, dst_ref=ref, send_sem=sem, recv_sem=sem,
        device_id={axis: peer}, device_id_type=MESH,
    ).wait_recv()


def total_of(copies, own, recv):
    total = own
    for k in reversed(range(len(copies))):
        copies[k].wait_recv()
        total = total + recv[k].astype(F32)
    return total


def dot(a, b):
    return jnp.dot(a, b, preferred_element_type=F32)


def row_squares(h):
    return jnp.sum(h * h, axis=1, keepdims=True)


def squares_tile(h):
    s = row_squares(h)
    high = s.astype(BF16).astype(F32)
    lane = lax.broadcasted_iota(jnp.int32, (h.shape[0], LANES), 1)
    return jnp.where(lane < LANES // 2, high, s - high).astype(BF16)


def row_factor(tile, width):
    s = tile[:, :1] + tile[:, LANES // 2 : LANES // 2 + 1]
    return lax.rsqrt(s / width + EPS)


def feed_forward(n_kv, h, gain, w_gate, w_up, w_down, loads, scratch, sems, meanwhile):
    send, recv, act_own, act_all = scratch
    rs_send, rs_recv, ag_send, ag_recv = sems
    me = lax.axis_index("kv")
    hidden = w_gate.shape[1]
    cw = act_own.shape[1]
    tile = squares_tile(h)
    scaled = (h * gain).astype(BF16)
    loads[0].wait()
    loads[1].wait()
    for c in range(COL_GROUPS):
        low = c * cw
        w = min(cw, hidden - low)
        for base, weight in ((0, w_gate), (cw, w_up)):
            part = dot(scaled, weight[:, low : low + w])
            for r in range(ROW_GROUPS):
                rows = slice(r * TILE, (r + 1) * TILE)
                send[r * COL_GROUPS + c, :, base : base + w] = part[rows].astype(BF16)
                if w < cw:
                    send[r * COL_GROUPS + c, :, base + w : base + cw] = jnp.zeros(
                        (TILE, cw - w), BF16
                    )
        for r in range(ROW_GROUPS):
            send[r * COL_GROUPS + c, :, 2 * cw :] = tile[r * TILE : (r + 1) * TILE]
    copies = exchange(
        "kv", lambda d: send.at[d], lambda k: recv.at[k], rs_send, lambda k: rs_recv.at[k]
    )
    total = total_of(copies, send[me].astype(F32), recv)
    factor = row_factor(total[:, 2 * cw :], h.shape[1] * n_kv)
    gate = total[:, :cw] * factor
    up = total[:, cw : 2 * cw] * factor
    act = (gate / (1.0 + jnp.exp(-gate)) * up).astype(BF16)
    act_own[...] = act
    act_all[me] = act
    exchange("kv", lambda d: act_own, lambda k: act_all.at[me], ag_send, lambda k: ag_recv)
    meanwhile()
    loads[2].wait()
    drain("kv", act_all.at[pl.ds(0, n_kv - 1)], ag_recv)
    out = None
    for c in range(COL_GROUPS):
        low = c * cw
        w = min(cw, hidden - low)
        block = jnp.concatenate(
            [act_all[r * COL_GROUPS + c, :, :w].astype(F32) for r in range(ROW_GROUPS)], axis=0
        ).astype(BF16)
        term = dot(block, w_down[low : low + w, :])
        out = term if out is None else out + term
    return out


def sum_over_tp(part, send, recv, send_sem, recv_sems, meanwhile=None):
    send[...] = part.astype(BF16)
    copies = exchange(
        "tp", lambda d: send, lambda k: recv.at[k], send_sem, lambda k: recv_sems.at[k]
    )
    if meanwhile is not None:
        meanwhile()
    return total_of(copies, send[...].astype(F32), recv)


def query_step(n_kv, h, gain, w_query, q_send, q_recv, send_sem, recv_sems):
    rows = h.shape[0]
    product = dot((h * gain).astype(BF16), w_query[...])
    row = lax.broadcasted_iota(jnp.int32, (rows, LANES), 0)
    lane = lax.broadcasted_iota(jnp.int32, (rows, LANES), 1)
    s = jnp.sum(jnp.where(row == lane, row_squares(h), 0.0), axis=0, keepdims=True)
    high = s.astype(BF16).astype(F32)
    first = lax.broadcasted_iota(jnp.int32, (TILE, LANES), 0)
    stats = jnp.where(first == 0, high, jnp.where(first == 1, s - high, 0.0))
    tiles = rows // TILE
    for r in range(tiles):
        for c in range(2):
            q_send[2 * r + c] = product[
                r * TILE : (r + 1) * TILE, c * LANES : (c + 1) * LANES
            ].astype(BF16)
    q_send[2 * tiles] = stats.astype(BF16)
    copies = exchange(
        "kv", lambda d: q_send, lambda k: q_recv.at[k], send_sem, lambda k: recv_sems.at[k]
    )
    total = total_of(copies, q_send[...].astype(F32), q_recv)
    s = jnp.sum(total[2 * tiles], axis=0, keepdims=True)
    factor = lax.rsqrt(s / (h.shape[1] * n_kv) + EPS)
    factor = jnp.sum(jnp.where(row == lane, factor, 0.0), axis=1, keepdims=True)
    halves = [
        jnp.concatenate([total[2 * r + c] for r in range(tiles)], axis=0) * factor
        for c in range(2)
    ]
    low = lane < HEAD
    first_half = jnp.where(low, halves[0], pltpu.roll(halves[1], HEAD, 1))
    second_half = jnp.where(low, pltpu.roll(halves[0], HEAD, 1), halves[1])
    return first_half.astype(BF16), second_half.astype(BF16)


def spread_queries(q_parts, pairs, qx):
    batch = q_parts[0].shape[0]
    per = qx.shape[1]
    rows = pairs * per
    row = lax.broadcasted_iota(jnp.int32, (rows, batch), 0)
    col = lax.broadcasted_iota(jnp.int32, (rows, batch), 1)
    pick = jnp.where(col == row // per + pairs * lax.rem(row, 2), 1.0, 0.0).astype(BF16)
    wide_row = lax.broadcasted_iota(jnp.int32, (rows, LANES), 0)
    lane = lax.broadcasted_iota(jnp.int32, (rows, LANES), 1)
    which = lax.rem(wide_row // 2, 2)
    y = jnp.where(which == 0, dot(pick, q_parts[0]), dot(pick, q_parts[1]))
    mine = lane // (HEAD // MAPS) == lax.rem(wide_row // 4, 4)
    y = jnp.where(mine, y, 0.0)
    member = lax.rem(wide_row, 2)
    for i in range(2):
        block = jnp.where(member == i, y, 0.0).astype(BF16)
        qx[:, :, i * LANES : (i + 1) * LANES] = block.reshape(pairs, per, LANES)


def turn_keys(k_buf, k_turned, first, last):
    def body(p, carry):
        k_turned[p] = k_buf[p].T
        return carry

    lax.fori_loop(first, last, body, 0)


def attention_step(
    scale, qx, k_turned, v_buf, o_send, o_recv, st_send, st_recv, send_sems, recv_sems
):
    pairs = qx.shape[0]
    row = lax.broadcasted_iota(jnp.int32, (2 * TILE, LANES), 0)
    lane = lax.broadcasted_iota(jnp.int32, (TILE, LANES), 1)
    first_member = lax.rem(row, 2) == 0
    low = lane < HEAD
    stats = jnp.zeros((TILE, LANES), F32)
    ahead = dot(qx[0], k_turned[0])
    begin = 0
    for p in range(pairs):
        s = ahead
        if p + 1 < pairs:
            ahead = dot(qx[p + 1], k_turned[p + 1])
        peak = jnp.max(s, axis=1, keepdims=True)
        e = jnp.exp2((s - peak) * scale)
        l = jnp.sum(e, axis=1, keepdims=True)
        lse = peak * scale + jnp.log2(l)
        stats = jnp.where(lane == 2 * p, lse[:TILE], stats)
        stats = jnp.where(lane == 2 * p + 1, lse[TILE:], stats)
        o = dot(e.astype(BF16), v_buf[p]) / l
        o = jnp.where(first_member, o[:, :LANES], o[:, LANES:])
        o_send[p] = jnp.where(low, o[:TILE], o[TILE:]).astype(BF16)
        if p + 1 == pairs:
            st_send[...] = stats[:, : 2 * pairs]
            exchange(
                "kv", lambda d: st_send, lambda k: st_recv.at[k],
                send_sems.at[0], lambda k: recv_sems.at[0],
            )
        if p + 1 in GROUP_ENDS:
            span = pl.ds(begin, p + 1 - begin)
            at = GROUP_ENDS.index(p + 1) + 1
            exchange(
                "kv", lambda d: o_send.at[span], lambda k: o_recv.at[k, span],
                send_sems.at[at], lambda k: recv_sems.at[at],
            )
            begin = p + 1


def drain_groups(o_recv, sems):
    begin = 0
    for at, end in enumerate(GROUP_ENDS):
        drain("kv", o_recv.at[:, pl.ds(begin, end - begin)], sems.at[at + 1])
        begin = end


def selector(sel):
    depth, width = sel.shape
    for j in range(width // LANES):
        row = lax.broadcasted_iota(jnp.int32, (depth, LANES), 0)
        lane = lax.broadcasted_iota(jnp.int32, (depth, LANES), 1)
        count = width // HEAD
        here = lax.rem(row, count) == 2 * j + lane // HEAD
        sel[:, j * LANES : (j + 1) * LANES] = jnp.where(here, 1.0, 0.0).astype(BF16)


def head_weights(map_weight, group, kv_local):
    row = lax.broadcasted_iota(jnp.int32, (TILE, LANES), 0)
    lane = lax.broadcasted_iota(jnp.int32, (TILE, LANES), 1)
    weight = jnp.zeros((TILE, LANES), F32)
    for k in range(kv_local):
        for g in range(group):
            here = (lax.rem(row // 2, group) == g) & (lane // HEAD == k)
            at = k * group + g
            weight = jnp.where(here, map_weight[:, at : at + 1], weight)
    return weight


def merge_heads(o_send, o_recv, st_send, st_recv, recv_sems, sel, weight, gain, heads):
    pairs = o_send.shape[0]
    count = 2 * pairs
    others = st_recv.shape[0]
    lane = lax.broadcasted_iota(jnp.int32, (TILE, LANES), 1)
    drain("kv", st_recv, recv_sems.at[0])
    lses = [st_send[...]] + [st_recv[k] for k in range(others)]
    peak = functools.reduce(jnp.maximum, lses)
    weights = [jnp.exp2(lse - peak) for lse in lses]
    share = 1.0 / functools.reduce(jnp.add, weights)
    compact = jnp.concatenate([w * share for w in weights], axis=0)
    high = compact.astype(BF16)
    rest = (compact - high.astype(F32)).astype(BF16)
    spread = jnp.concatenate([high, rest], axis=1)
    drain_groups(o_recv, recv_sems)
    low = lane < HEAD
    for j in range(pairs // 2):
        wide = dot(spread, sel[:, 2 * j * LANES : 2 * (j + 1) * LANES])
        for i in range(2):
            p = 2 * j + i
            columns = slice(i * LANES, (i + 1) * LANES)
            outs = [o_send[p].astype(F32)] + [o_recv[k, p].astype(F32) for k in range(others)]
            merged = functools.reduce(
                jnp.add,
                [wide[d * TILE : (d + 1) * TILE, columns] * o for d, o in enumerate(outs)],
            )
            diff = merged - weight * pltpu.roll(merged, TILE // 2, 0)
            square = diff * diff
            left = jnp.sum(jnp.where(low, square, 0.0), axis=1, keepdims=True)
            right = jnp.sum(jnp.where(low, 0.0, square), axis=1, keepdims=True)
            mean = jnp.where(low, left, right) / HEAD
            heads[p * TILE : (p + 1) * TILE, :] = diff * lax.rsqrt(mean + EPS) * gain


def start_loads(pairs, sems):
    loads = [pltpu.make_async_copy(a, b, sems.at[i]) for i, (a, b) in enumerate(pairs)]
    for load in loads:
        load.start()
    return loads


def layer_kernel(
    n_kv, n_tp, kv_local, group, scale,
    tokens_any, gain1_any, gain_mix_any, gain2_any, weight_any, head_gain_any,
    gate1_any, up1_any, down1_any, query_any, key_any, value_any, out_any,
    gate2_any, up2_any, down2_any,
    mixed,
    tokens, first_gain, mix_gain, second_gain, map_weight, head_gain,
    w_gate1, w_up1, w_down1, w_query, k_buf, k_turned, v_buf, w_out, w_gate2, w_up2, w_down2,
    tok_all, rs1_send, rs1_recv, act1_own, act1_all, tp1_send, tp1_recv, q_send, q_recv, qx,
    o_send, o_recv, st_send, st_recv, sel, head_all, tp2_send, tp2_recv,
    rs2_send, rs2_recv, act2_own, act2_all, fin_send, fin_recv,
    small_sems, load_sems, cache_sems, send_sems, once_sems, kv_sems, tp1_sems, tp2_sems,
    o_send_sems, o_recv_sems,
):
    pairs = k_buf.shape[0]
    small = start_loads(
        (
            (tokens_any, tokens),
            (gain1_any, first_gain),
            (gain_mix_any, mix_gain),
            (gain2_any, second_gain),
            (weight_any, map_weight),
            (head_gain_any, head_gain),
        ),
        small_sems,
    )
    loads = start_loads(
        (
            (gate1_any, w_gate1),
            (up1_any, w_up1),
            (down1_any, w_down1),
            (query_any, w_query),
            (gate2_any, w_gate2),
            (up2_any, w_up2),
            (down2_any, w_down2),
        )
        + tuple(
            (
                out_any.at[pl.ds((k * group + g) * HEAD, HEAD)],
                w_out.at[pl.ds((g * kv_local + k) * HEAD, HEAD)],
            )
            for k in range(kv_local)
            for g in range(group)
        ),
        load_sems,
    )
    greet()
    cache_loads = start_loads(
        (
            (key_any.at[:pairs], k_buf.at[:, :, :LANES]),
            (key_any.at[pairs:], k_buf.at[:, :, LANES:]),
            (value_any.at[:pairs], v_buf.at[:, :, :LANES]),
            (value_any.at[pairs:], v_buf.at[:, :, LANES:]),
        ),
        cache_sems,
    )
    for load in small:
        load.wait()
    tp = lax.axis_index("tp")
    tok_all[tp] = tokens[...]
    exchange(
        "tp", lambda d: tokens, lambda k: tok_all.at[tp], send_sems.at[0], lambda k: once_sems.at[0]
    )
    selector(sel)
    drain("tp", tok_all.at[pl.ds(0, n_tp - 1)], once_sems.at[0])
    h = jnp.concatenate([tok_all[j].astype(F32) for j in range(n_tp)], axis=1)

    def keys_first():
        cache_loads[0].wait()
        cache_loads[1].wait()
        turn_keys(k_buf, k_turned, 0, pairs // 2)

    def keys_second():
        turn_keys(k_buf, k_turned, pairs // 2, pairs)

    part = feed_forward(
        n_kv, h, first_gain[...], w_gate1, w_up1, w_down1, loads[:3],
        (rs1_send, rs1_recv, act1_own, act1_all),
        (send_sems.at[1], kv_sems, send_sems.at[2], once_sems.at[1]),
        keys_first,
    )
    h = h + 0.5 * sum_over_tp(part, tp1_send, tp1_recv, send_sems.at[3], tp1_sems, keys_second)
    loads[3].wait()
    q_parts = query_step(
        n_kv, h, mix_gain[...], w_query, q_send, q_recv, send_sems.at[4], kv_sems
    )
    spread_queries(q_parts, pairs, qx)
    cache_loads[2].wait()
    cache_loads[3].wait()
    attention_step(
        scale, qx, k_turned, v_buf, o_send, o_recv, st_send, st_recv, o_send_sems, o_recv_sems
    )
    weight = head_weights(map_weight, group, kv_local)
    gain = jnp.concatenate([head_gain[...] * HEAD_SCALE] * kv_local, axis=1)
    merge_heads(o_send, o_recv, st_send, st_recv, o_recv_sems, sel, weight, gain, head_all)
    heads = jnp.concatenate(
        [
            jnp.concatenate(
                [head_all[pl.ds(2 * g + i, pairs, stride=TILE), :] for g in range(group)], axis=1
            )
            for i in range(2)
        ],
        axis=0,
    ).astype(BF16)
    for load in loads[7:]:
        load.wait()
    h = h + sum_over_tp(dot(heads, w_out[...]), tp2_send, tp2_recv, send_sems.at[5], tp2_sems)
    part = feed_forward(
        n_kv, h, second_gain[...], w_gate2, w_up2, w_down2, loads[4:7],
        (rs2_send, rs2_recv, act2_own, act2_all),
        (send_sems.at[6], kv_sems, send_sems.at[7], once_sems.at[2]),
        lambda: None,
    )
    batch, width = mixed.shape
    own = jnp.zeros((batch, width), F32)
    for j in range(n_tp):
        columns = slice(j * width, (j + 1) * width)
        fin_send[j] = part[:, columns].astype(BF16)
        own = jnp.where(tp == j, h[:, columns], own)
    copies = exchange(
        "tp", lambda d: fin_send.at[d], lambda k: fin_recv.at[k],
        send_sems.at[8], lambda k: tp1_sems.at[k],
    )
    drain("tp", tok_all.at[pl.ds(0, n_tp - 1)], send_sems.at[0])
    drain("kv", rs1_recv, send_sems.at[1])
    drain("kv", act1_all.at[pl.ds(0, n_kv - 1)], send_sems.at[2])
    drain("tp", tp1_recv, send_sems.at[3])
    drain("kv", q_recv, send_sems.at[4])
    drain("kv", st_recv, o_send_sems.at[0])
    drain_groups(o_recv, o_send_sems)
    drain("tp", tp2_recv, send_sems.at[5])
    drain("kv", rs2_recv, send_sems.at[6])
    drain("kv", act2_all.at[pl.ds(0, n_kv - 1)], send_sems.at[7])
    total = total_of(copies, fin_send[tp].astype(F32), fin_recv)
    drain("tp", fin_recv, send_sems.at[8])
    mixed[...] = (own + 0.5 * total).astype(BF16)


def on_device(
    n_kv, n_tp, tokens, first_gain, first_gate, first_up, first_down, mix_gain, w_query,
    key_cache, value_cache, map_weight, head_gain, w_out, second_gain, second_gate, second_up,
    second_down,
):
    batch, own_width = tokens.shape
    depth, hidden = first_gate.shape
    length = key_cache.shape[1]
    columns = w_query.shape[1]
    kv_local = key_cache.shape[2] // HEAD
    group = columns // (kv_local * HEAD)
    pairs = batch // 2
    cw = -(-hidden // (LANES * COL_GROUPS)) * LANES
    hbm = pl.BlockSpec(memory_space=pl.ANY)
    ffn_buffers = [
        pltpu.VMEM((n_kv, TILE, 2 * cw + LANES), BF16),
        pltpu.VMEM((n_kv - 1, TILE, 2 * cw + LANES), BF16),
        pltpu.VMEM((TILE, cw), BF16),
        pltpu.VMEM((n_kv, TILE, cw), BF16),
    ]
    tp_buffers = [pltpu.VMEM((batch, depth), BF16), pltpu.VMEM((n_tp - 1, batch, depth), BF16)]
    q_tiles = 2 * (batch // TILE) + 1
    return pl.pallas_call(
        functools.partial(
            layer_kernel, n_kv, n_tp, kv_local, group, math.log2(math.e) / math.sqrt(HEAD // MAPS)
        ),
        out_shape=pltpu.VMEM((batch, depth // n_tp), BF16),
        in_specs=[hbm] * 16,
        out_specs=pl.BlockSpec(memory_space=pltpu.VMEM),
        scratch_shapes=[
            pltpu.VMEM(tokens.shape, BF16),
            pltpu.VMEM((1, depth), F32),
            pltpu.VMEM((1, depth), F32),
            pltpu.VMEM((1, depth), F32),
            pltpu.VMEM((1, kv_local * group), F32),
            pltpu.VMEM((1, HEAD), F32),
            pltpu.VMEM(first_gate.shape, BF16),
            pltpu.VMEM(first_up.shape, BF16),
            pltpu.VMEM(first_down.shape, BF16),
            pltpu.VMEM(w_query.shape, BF16),
            pltpu.VMEM((pairs, length, 2 * LANES), BF16),
            pltpu.VMEM((pairs, 2 * LANES, length), BF16),
            pltpu.VMEM((pairs, length, 2 * LANES), BF16),
            pltpu.VMEM(w_out.shape, BF16),
            pltpu.VMEM(second_gate.shape, BF16),
            pltpu.VMEM(second_up.shape, BF16),
            pltpu.VMEM(second_down.shape, BF16),
            pltpu.VMEM((n_tp,) + tokens.shape, BF16),
            *ffn_buffers,
            *tp_buffers,
            pltpu.VMEM((q_tiles, TILE, LANES), BF16),
            pltpu.VMEM((n_kv - 1, q_tiles, TILE, LANES), BF16),
            pltpu.VMEM((pairs, 2 * TILE, 2 * LANES), BF16),
            pltpu.VMEM((pairs, TILE, LANES), BF16),
            pltpu.VMEM((n_kv - 1, pairs, TILE, LANES), BF16),
            pltpu.VMEM((TILE, 2 * pairs), F32),
            pltpu.VMEM((n_kv - 1, TILE, 2 * pairs), F32),
            pltpu.VMEM((4 * pairs, pairs * LANES), BF16),
            pltpu.VMEM((pairs * TILE, LANES), F32),
            *tp_buffers,
            *ffn_buffers,
            pltpu.VMEM((n_tp, batch, own_width), BF16),
            pltpu.VMEM((n_tp - 1, batch, own_width), BF16),
            pltpu.SemaphoreType.DMA((6,)),
            pltpu.SemaphoreType.DMA((7 + kv_local * group,)),
            pltpu.SemaphoreType.DMA((4,)),
            pltpu.SemaphoreType.DMA((9,)),
            pltpu.SemaphoreType.DMA((3,)),
            pltpu.SemaphoreType.DMA((n_kv - 1,)),
            pltpu.SemaphoreType.DMA((n_tp - 1,)),
            pltpu.SemaphoreType.DMA((n_tp - 1,)),
            pltpu.SemaphoreType.DMA((len(GROUP_ENDS) + 1,)),
            pltpu.SemaphoreType.DMA((len(GROUP_ENDS) + 1,)),
        ],
        compiler_params=pltpu.CompilerParams(
            collective_id=1, has_side_effects=True, vmem_limit_bytes=VMEM_LIMIT
        ),
    )(
        tokens, first_gain.reshape(1, -1), mix_gain.reshape(1, -1), second_gain.reshape(1, -1),
        map_weight.reshape(1, -1), head_gain.reshape(1, -1),
        first_gate, first_up, first_down, w_query, key_cache, value_cache, w_out,
        second_gate, second_up, second_down,
    )


def solution(mesh):
    placed = (
        P(None, ("kv", "tp")),
        P("kv"),
        P("kv", "tp"),
        P("kv", "tp"),
        P("tp", "kv"),
        P("kv"),
        P("kv", "tp"),
        P(None, "kv", "tp"),
        P(None, "kv", "tp"),
        P("tp"),
        P(),
        P("tp", "kv"),
        P("kv"),
        P("kv", "tp"),
        P("kv", "tp"),
        P("tp", "kv"),
    )
    return jax.shard_map(
        functools.partial(on_device, mesh.shape["kv"], mesh.shape["tp"]),
        mesh=mesh,
        in_specs=placed,
        out_specs=P(None, ("kv", "tp")),
        check_vma=False,
    )
```

```python
import functools
import math

import jax
import jax.numpy as jnp
from jax import lax
from jax.experimental import pallas as pl
from jax.experimental.pallas import tpu as pltpu
from jax.sharding import PartitionSpec as P

HEAD = 64
MAPS = 2
LANES = 128
TILE = 8
EPS = 1e-06
HEAD_SCALE = 0.8
SIDE = 4
STEPS = (2, 1, 3, 0)
ROW_GROUPS = 4
COL_GROUPS = 4
F32 = jnp.float32
BF16 = jnp.bfloat16
MESH = pl.DeviceIdType.MESH
VMEM_LIMIT = 60 * 1024 * 1024


def hops(d):
    return min(d, SIDE - d)


def kv_offsets():
    offs = [(a, b) for a in range(SIDE) for b in range(SIDE) if (a, b) != (0, 0)]
    return sorted(offs, key=lambda o: -(hops(o[0]) + hops(o[1])))


def tp_offsets():
    offs = [(a, b) for a in range(SIDE) for b in range(2) if (a, b) != (0, 0)]
    return sorted(offs, key=lambda o: -(2 * hops(o[0]) + o[1]))


def shifted(axis, offset):
    me = lax.axis_index(axis)
    inner = SIDE if axis == "kv" else 2
    high = lax.rem(me // inner + offset[0], SIDE)
    low = lax.rem(lax.rem(me, inner) + offset[1], inner)
    return high * inner + low


OFFSETS = {"kv": kv_offsets(), "tp": tp_offsets()}


def greet():
    barrier = pltpu.get_barrier_semaphore()
    total = 0
    for axis in ("kv", "tp"):
        for offset in OFFSETS[axis]:
            pl.semaphore_signal(
                barrier, inc=1, device_id={axis: shifted(axis, offset)}, device_id_type=MESH
            )
            total += 1
    pl.semaphore_wait(barrier, total)


def exchange(axis, source, target, send_sem, recv_sem):
    copies = []
    for k, offset in enumerate(OFFSETS[axis]):
        dest = shifted(axis, offset)
        copy = pltpu.make_async_remote_copy(
            src_ref=source(dest),
            dst_ref=target(k),
            send_sem=send_sem,
            recv_sem=recv_sem(k),
            device_id={axis: dest},
            device_id_type=MESH,
        )
        copy.start()
        copies.append(copy)
    return copies


def drain(axis, ref, sem):
    peer = shifted(axis, OFFSETS[axis][0])
    pltpu.make_async_remote_copy(
        src_ref=ref, dst_ref=ref, send_sem=sem, recv_sem=sem,
        device_id={axis: peer}, device_id_type=MESH,
    ).wait_recv()


def total_of(copies, own, recv):
    total = own
    for k in reversed(range(len(copies))):
        copies[k].wait_recv()
        total = total + recv[k].astype(F32)
    return total


def dot(a, b):
    return jnp.dot(a, b, preferred_element_type=F32)


def row_squares(h):
    return jnp.sum(h * h, axis=1, keepdims=True)


def squares_tile(h):
    s = row_squares(h)
    high = s.astype(BF16).astype(F32)
    lane = lax.broadcasted_iota(jnp.int32, (h.shape[0], LANES), 1)
    return jnp.where(lane < LANES // 2, high, s - high).astype(BF16)


def row_factor(tile, width):
    s = tile[:, :1] + tile[:, LANES // 2 : LANES // 2 + 1]
    return lax.rsqrt(s / width + EPS)


def feed_forward(n_kv, h, gain, w_gate, w_up, w_down, loads, scratch, sems, meanwhile):
    send, recv, act_own, act_all = scratch
    rs_send, rs_recv, ag_send, ag_recv = sems
    me = lax.axis_index("kv")
    hidden = w_down.shape[0]
    cw = act_own.shape[1]
    tile = squares_tile(h)
    scaled = (h * gain).astype(BF16)
    loads[0].wait()
    loads[1].wait()

    def product(c):
        columns = pl.ds(pl.multiple_of(c * cw, LANES), cw)
        return dot(scaled, jnp.concatenate([w_gate[:, columns], w_up[:, columns]], axis=1))

    z, y = me // SIDE, lax.rem(me, SIDE)
    groups = [lax.rem(y + step, SIDE) for step in STEPS]
    copies = [None] * len(OFFSETS["kv"])
    ahead = product(groups[0])
    for at, step in enumerate(STEPS):
        c, part = groups[at], ahead
        if at + 1 < len(STEPS):
            ahead = product(groups[at + 1])
        for r in range(ROW_GROUPS):
            rows = slice(r * TILE, (r + 1) * TILE)
            send[r * COL_GROUPS + c, :, : 2 * cw] = part[rows].astype(BF16)
            send[r * COL_GROUPS + c, :, 2 * cw :] = tile[rows]
        for up in STEPS:
            if (up, step) == (0, 0):
                continue
            k = OFFSETS["kv"].index((up, step))
            dest = lax.rem(z + up, SIDE) * SIDE + c
            copies[k] = pltpu.make_async_remote_copy(
                src_ref=send.at[dest], dst_ref=recv.at[k],
                send_sem=rs_send, recv_sem=rs_recv.at[k],
                device_id={"kv": dest}, device_id_type=MESH,
            )
            copies[k].start()
    total = total_of(copies, send[me].astype(F32), recv)
    factor = row_factor(total[:, 2 * cw :], h.shape[1] * n_kv)
    gate = total[:, :cw] * factor
    up = total[:, cw : 2 * cw] * factor
    act = (gate / (1.0 + jnp.exp(-gate)) * up).astype(BF16)
    act_own[...] = act
    act_all[me] = act
    exchange("kv", lambda d: act_own, lambda k: act_all.at[me], ag_send, lambda k: ag_recv)
    meanwhile()
    loads[2].wait()
    drain("kv", act_all.at[pl.ds(0, n_kv - 1)], ag_recv)
    out = None
    for c in range(COL_GROUPS):
        low = c * cw
        w = min(cw, hidden - low)
        block = jnp.concatenate(
            [act_all[r * COL_GROUPS + c, :, :w].astype(F32) for r in range(ROW_GROUPS)], axis=0
        ).astype(BF16)
        term = dot(block, w_down[low : low + w, :])
        out = term if out is None else out + term
    return out


def sum_over_tp(part, send, recv, send_sem, recv_sems, meanwhile=None):
    send[...] = part.astype(BF16)
    copies = exchange(
        "tp", lambda d: send, lambda k: recv.at[k], send_sem, lambda k: recv_sems.at[k]
    )
    if meanwhile is not None:
        meanwhile()
    return total_of(copies, send[...].astype(F32), recv)


def query_step(n_kv, h, gain, w_query, q_send, q_recv, send_sems, recv_sems):
    rows = h.shape[0]
    product = dot((h * gain).astype(BF16), w_query[...])
    row = lax.broadcasted_iota(jnp.int32, (rows, LANES), 0)
    lane = lax.broadcasted_iota(jnp.int32, (rows, LANES), 1)
    s = jnp.sum(jnp.where(row == lane, row_squares(h), 0.0), axis=0, keepdims=True)
    high = s.astype(BF16).astype(F32)
    first = lax.broadcasted_iota(jnp.int32, (TILE, LANES), 0)
    stats = jnp.where(first == 0, high, jnp.where(first == 1, s - high, 0.0))
    per = rows // TILE // 2
    count = 2 * per
    starts = (0, count + 1)
    spans = (pl.ds(0, count + 1), pl.ds(count + 1, count))
    for half in range(2):
        for r in range(per):
            for c in range(2):
                at = (half * per + r) * TILE
                q_send[starts[half] + 2 * r + c] = product[
                    at : at + TILE, c * LANES : (c + 1) * LANES
                ].astype(BF16)
    q_send[count] = stats.astype(BF16)
    rounds = [
        exchange(
            "kv", lambda d: q_send.at[spans[half]], lambda k: q_recv.at[k, spans[half]],
            send_sems[half], lambda k: recv_sems[half].at[k],
        )
        for half in range(2)
    ]

    def finish(half, factor):
        total = total_of(
            rounds[half], q_send[spans[half]].astype(F32), q_recv.at[:, spans[half]]
        )
        if half == 0:
            s = jnp.sum(total[count], axis=0, keepdims=True)
            factor = lax.rsqrt(s / (h.shape[1] * n_kv) + EPS)
            factor = jnp.sum(jnp.where(row == lane, factor, 0.0), axis=1, keepdims=True)
        mine = factor[half * per * TILE : (half + 1) * per * TILE]
        parts = [
            jnp.concatenate([total[2 * r + c] for r in range(per)], axis=0) * mine
            for c in range(2)
        ]
        low = lane[: per * TILE] < HEAD
        first_half = jnp.where(low, parts[0], pltpu.roll(parts[1], HEAD, 1))
        second_half = jnp.where(low, pltpu.roll(parts[0], HEAD, 1), parts[1])
        return (first_half.astype(BF16), second_half.astype(BF16)), factor

    return finish


def spread_queries(q_parts, qx, begin, count):
    batch = q_parts[0].shape[0]
    per = qx.shape[1]
    rows = count * per
    row = lax.broadcasted_iota(jnp.int32, (rows, batch), 0)
    col = lax.broadcasted_iota(jnp.int32, (rows, batch), 1)
    pick = jnp.where(col == row // per + count * lax.rem(row, 2), 1.0, 0.0).astype(BF16)
    wide_row = lax.broadcasted_iota(jnp.int32, (rows, LANES), 0)
    lane = lax.broadcasted_iota(jnp.int32, (rows, LANES), 1)
    which = lax.rem(wide_row // 2, 2)
    y = jnp.where(which == 0, dot(pick, q_parts[0]), dot(pick, q_parts[1]))
    mine = lane // (HEAD // MAPS) == lax.rem(wide_row // 4, 4)
    y = jnp.where(mine, y, 0.0)
    member = lax.rem(wide_row, 2)
    for i in range(2):
        block = jnp.where(member == i, y, 0.0).astype(BF16)
        qx[begin : begin + count, :, i * LANES : (i + 1) * LANES] = block.reshape(
            count, per, LANES
        )


def turn_keys(k_buf, k_turned, first, last):
    def body(p, carry):
        k_turned[p] = k_buf[p].T
        return carry

    lax.fori_loop(first, last, body, 0)


def attention_step(scale, qx, k_turned, v_buf, begin, end, stats, o_send):
    row = lax.broadcasted_iota(jnp.int32, (2 * TILE, LANES), 0)
    lane = lax.broadcasted_iota(jnp.int32, (TILE, LANES), 1)
    first_member = lax.rem(row, 2) == 0
    low = lane < HEAD
    ahead = dot(qx[begin], k_turned[begin])
    for p in range(begin, end):
        s = ahead
        if p + 1 < end:
            ahead = dot(qx[p + 1], k_turned[p + 1])
        peak = jnp.max(s, axis=1, keepdims=True)
        e = jnp.exp2((s - peak) * scale)
        l = jnp.sum(e, axis=1, keepdims=True)
        lse = peak * scale + jnp.log2(l)
        stats = jnp.where(lane == 2 * p, lse[:TILE], stats)
        stats = jnp.where(lane == 2 * p + 1, lse[TILE:], stats)
        o = dot(e.astype(BF16), v_buf[p]) / l
        o = jnp.where(first_member, o[:, :LANES], o[:, LANES:])
        o_send[p] = jnp.where(low, o[:TILE], o[TILE:]).astype(BF16)
    return stats


def drain_groups(o_recv, sems):
    half = o_recv.shape[1] // 2
    for i in range(2):
        drain("kv", o_recv.at[:, pl.ds(i * half, half)], sems.at[i + 1])


def selector(sel):
    depth, width = sel.shape
    for j in range(width // LANES):
        row = lax.broadcasted_iota(jnp.int32, (depth, LANES), 0)
        lane = lax.broadcasted_iota(jnp.int32, (depth, LANES), 1)
        count = width // HEAD
        here = lax.rem(row, count) == 2 * j + lane // HEAD
        sel[:, j * LANES : (j + 1) * LANES] = jnp.where(here, 1.0, 0.0).astype(BF16)


def head_weights(map_weight, group, kv_local):
    row = lax.broadcasted_iota(jnp.int32, (TILE, LANES), 0)
    lane = lax.broadcasted_iota(jnp.int32, (TILE, LANES), 1)
    weight = jnp.zeros((TILE, LANES), F32)
    for k in range(kv_local):
        for g in range(group):
            here = (lax.rem(row // 2, group) == g) & (lane // HEAD == k)
            at = k * group + g
            weight = jnp.where(here, map_weight[:, at : at + 1], weight)
    return weight


def merge_heads(o_send, o_recv, st_send, st_recv, recv_sems, sel, weight, gain, heads):
    pairs = o_send.shape[0]
    count = 2 * pairs
    others = st_recv.shape[0]
    lane = lax.broadcasted_iota(jnp.int32, (TILE, LANES), 1)
    drain("kv", st_recv, recv_sems.at[0])
    lses = [st_send[...]] + [st_recv[k] for k in range(others)]
    peak = functools.reduce(jnp.maximum, lses)
    weights = [jnp.exp2(lse - peak) for lse in lses]
    share = 1.0 / functools.reduce(jnp.add, weights)
    compact = jnp.concatenate([w * share for w in weights], axis=0)
    high = compact.astype(BF16)
    rest = (compact - high.astype(F32)).astype(BF16)
    spread = jnp.concatenate([high, rest], axis=1)
    drain_groups(o_recv, recv_sems)
    low = lane < HEAD
    for j in range(pairs // 2):
        wide = dot(spread, sel[:, 2 * j * LANES : 2 * (j + 1) * LANES])
        for i in range(2):
            p = 2 * j + i
            columns = slice(i * LANES, (i + 1) * LANES)
            outs = [o_send[p].astype(F32)] + [o_recv[k, p].astype(F32) for k in range(others)]
            merged = functools.reduce(
                jnp.add,
                [wide[d * TILE : (d + 1) * TILE, columns] * o for d, o in enumerate(outs)],
            )
            diff = merged - weight * pltpu.roll(merged, TILE // 2, 0)
            square = diff * diff
            left = jnp.sum(jnp.where(low, square, 0.0), axis=1, keepdims=True)
            right = jnp.sum(jnp.where(low, 0.0, square), axis=1, keepdims=True)
            mean = jnp.where(low, left, right) / HEAD
            heads[p * TILE : (p + 1) * TILE, :] = diff * lax.rsqrt(mean + EPS) * gain


def start_loads(pairs, sems):
    loads = [pltpu.make_async_copy(a, b, sems.at[i]) for i, (a, b) in enumerate(pairs)]
    for load in loads:
        load.start()
    return loads


def layer_kernel(
    n_kv, n_tp, kv_local, group, scale,
    tokens_any, gain1_any, gain_mix_any, gain2_any, weight_any, head_gain_any,
    gate1_any, up1_any, down1_any, query_any, key_any, value_any, out_any,
    gate2_any, up2_any, down2_any,
    mixed,
    tokens, first_gain, mix_gain, second_gain, map_weight, head_gain,
    w_gate1, w_up1, w_down1, w_query, k_buf, k_turned, v_buf, w_out, w_gate2, w_up2, w_down2,
    tok_all, rs1_send, rs1_recv, act1_own, act1_all, tp1_send, tp1_recv, q_send, q_recv, qx,
    o_send, o_recv, st_send, st_recv, sel, head_all, tp2_send, tp2_recv,
    rs2_send, rs2_recv, act2_own, act2_all, fin_send, fin_recv,
    small_sems, load_sems, cache_sems, send_sems, once_sems, kv_sems, second_sems, tp1_sems, tp2_sems,
    o_send_sems, o_recv_sems,
):
    pairs = k_buf.shape[0]
    half = pairs // 2
    hidden = w_down1.shape[0]
    small = start_loads(
        (
            (tokens_any, tokens),
            (gain1_any, first_gain),
            (gain_mix_any, mix_gain),
            (gain2_any, second_gain),
            (weight_any, map_weight),
            (head_gain_any, head_gain),
        ),
        small_sems,
    )
    loads = start_loads(
        (
            (gate1_any, w_gate1.at[:, pl.ds(0, hidden)]),
            (up1_any, w_up1.at[:, pl.ds(0, hidden)]),
            (down1_any, w_down1),
            (query_any, w_query),
            (gate2_any, w_gate2.at[:, pl.ds(0, hidden)]),
            (up2_any, w_up2.at[:, pl.ds(0, hidden)]),
            (down2_any, w_down2),
        )
        + tuple(
            (
                out_any.at[pl.ds((k * group + g) * HEAD, HEAD)],
                w_out.at[pl.ds((g * kv_local + k) * HEAD, HEAD)],
            )
            for k in range(kv_local)
            for g in range(group)
        ),
        load_sems,
    )
    if hidden < w_gate1.shape[1]:
        for weight in (w_gate1, w_up1, w_gate2, w_up2):
            weight[:, hidden:] = jnp.zeros((weight.shape[0], weight.shape[1] - hidden), BF16)
    greet()
    cache_loads = start_loads(
        tuple(
            (cache.at[pl.ds((2 * a + i) * half, half)], buf.at[pl.ds(a * half, half), :, lanes])
            for cache, buf in ((key_any, k_buf), (value_any, v_buf))
            for a in range(2)
            for i, lanes in enumerate((pl.ds(0, LANES), pl.ds(LANES, LANES)))
        ),
        cache_sems,
    )
    for load in small:
        load.wait()
    tp = lax.axis_index("tp")
    tok_all[tp] = tokens[...]
    exchange(
        "tp", lambda d: tokens, lambda k: tok_all.at[tp], send_sems.at[0], lambda k: once_sems.at[0]
    )
    selector(sel)
    drain("tp", tok_all.at[pl.ds(0, n_tp - 1)], once_sems.at[0])
    h = jnp.concatenate([tok_all[j].astype(F32) for j in range(n_tp)], axis=1)

    def keys_first():
        cache_loads[0].wait()
        cache_loads[1].wait()
        turn_keys(k_buf, k_turned, 0, half)

    def keys_second():
        cache_loads[2].wait()
        cache_loads[3].wait()
        turn_keys(k_buf, k_turned, half, pairs)

    part = feed_forward(
        n_kv, h, first_gain[...], w_gate1, w_up1, w_down1, loads[:3],
        (rs1_send, rs1_recv, act1_own, act1_all),
        (send_sems.at[1], kv_sems, send_sems.at[2], once_sems.at[1]),
        keys_first,
    )
    h = h + 0.5 * sum_over_tp(part, tp1_send, tp1_recv, send_sems.at[3], tp1_sems, keys_second)
    loads[3].wait()
    finish = query_step(
        n_kv, h, mix_gain[...], w_query, q_send, q_recv,
        (send_sems.at[4], send_sems.at[9]), (kv_sems, second_sems),
    )
    stats = jnp.zeros((TILE, LANES), F32)
    factor = None
    for a in range(2):
        q_parts, factor = finish(a, factor)
        begin, end = a * half, (a + 1) * half
        spread_queries(q_parts, qx, begin, half)
        cache_loads[4 + 2 * a].wait()
        cache_loads[5 + 2 * a].wait()
        stats = attention_step(scale, qx, k_turned, v_buf, begin, end, stats, o_send)
        if a == 1:
            st_send[...] = stats[:, : 2 * pairs]
            exchange(
                "kv", lambda d: st_send, lambda k: st_recv.at[k],
                o_send_sems.at[0], lambda k: o_recv_sems.at[0],
            )
        span = pl.ds(begin, half)
        exchange(
            "kv", lambda d: o_send.at[span], lambda k: o_recv.at[k, span],
            o_send_sems.at[a + 1], lambda k: o_recv_sems.at[a + 1],
        )
    weight = head_weights(map_weight, group, kv_local)
    gain = jnp.concatenate([head_gain[...] * HEAD_SCALE] * kv_local, axis=1)
    merge_heads(o_send, o_recv, st_send, st_recv, o_recv_sems, sel, weight, gain, head_all)
    heads = jnp.concatenate(
        [
            jnp.concatenate(
                [
                    head_all[pl.ds(a * half * TILE + 2 * g + i, half, stride=TILE), :]
                    for g in range(group)
                ],
                axis=1,
            )
            for a in range(2)
            for i in range(2)
        ],
        axis=0,
    ).astype(BF16)
    for load in loads[7:]:
        load.wait()
    h = h + sum_over_tp(dot(heads, w_out[...]), tp2_send, tp2_recv, send_sems.at[5], tp2_sems)
    part = feed_forward(
        n_kv, h, second_gain[...], w_gate2, w_up2, w_down2, loads[4:7],
        (rs2_send, rs2_recv, act2_own, act2_all),
        (send_sems.at[6], kv_sems, send_sems.at[7], once_sems.at[2]),
        lambda: None,
    )
    batch, width = mixed.shape
    own = jnp.zeros((batch, width), F32)
    for j in range(n_tp):
        columns = slice(j * width, (j + 1) * width)
        fin_send[j] = part[:, columns].astype(BF16)
        own = jnp.where(tp == j, h[:, columns], own)
    copies = exchange(
        "tp", lambda d: fin_send.at[d], lambda k: fin_recv.at[k],
        send_sems.at[8], lambda k: tp1_sems.at[k],
    )
    drain("tp", tok_all.at[pl.ds(0, n_tp - 1)], send_sems.at[0])
    drain("kv", rs1_recv, send_sems.at[1])
    drain("kv", act1_all.at[pl.ds(0, n_kv - 1)], send_sems.at[2])
    drain("tp", tp1_recv, send_sems.at[3])
    split = q_recv.shape[1] // 2 + 1
    drain("kv", q_recv.at[:, pl.ds(0, split)], send_sems.at[4])
    drain("kv", q_recv.at[:, pl.ds(split, split - 1)], send_sems.at[9])
    drain("kv", st_recv, o_send_sems.at[0])
    drain_groups(o_recv, o_send_sems)
    drain("tp", tp2_recv, send_sems.at[5])
    drain("kv", rs2_recv, send_sems.at[6])
    drain("kv", act2_all.at[pl.ds(0, n_kv - 1)], send_sems.at[7])
    total = total_of(copies, fin_send[tp].astype(F32), fin_recv)
    drain("tp", fin_recv, send_sems.at[8])
    mixed[...] = (own + 0.5 * total).astype(BF16)


def on_device(
    n_kv, n_tp, tokens, first_gain, first_gate, first_up, first_down, mix_gain, w_query,
    key_cache, value_cache, map_weight, head_gain, w_out, second_gain, second_gate, second_up,
    second_down,
):
    batch, own_width = tokens.shape
    depth, hidden = first_gate.shape
    length = key_cache.shape[1]
    columns = w_query.shape[1]
    kv_local = key_cache.shape[2] // HEAD
    group = columns // (kv_local * HEAD)
    pairs = batch // 2
    cw = -(-hidden // (LANES * COL_GROUPS)) * LANES
    hbm = pl.BlockSpec(memory_space=pl.ANY)
    ffn_buffers = [
        pltpu.VMEM((n_kv, TILE, 2 * cw + LANES), BF16),
        pltpu.VMEM((n_kv - 1, TILE, 2 * cw + LANES), BF16),
        pltpu.VMEM((TILE, cw), BF16),
        pltpu.VMEM((n_kv, TILE, cw), BF16),
    ]
    tp_buffers = [pltpu.VMEM((batch, depth), BF16), pltpu.VMEM((n_tp - 1, batch, depth), BF16)]
    q_tiles = 2 * (batch // TILE) + 1
    return pl.pallas_call(
        functools.partial(
            layer_kernel, n_kv, n_tp, kv_local, group, math.log2(math.e) / math.sqrt(HEAD // MAPS)
        ),
        out_shape=pltpu.VMEM((batch, depth // n_tp), BF16),
        in_specs=[hbm] * 16,
        out_specs=pl.BlockSpec(memory_space=pltpu.VMEM),
        scratch_shapes=[
            pltpu.VMEM(tokens.shape, BF16),
            pltpu.VMEM((1, depth), F32),
            pltpu.VMEM((1, depth), F32),
            pltpu.VMEM((1, depth), F32),
            pltpu.VMEM((1, kv_local * group), F32),
            pltpu.VMEM((1, HEAD), F32),
            pltpu.VMEM((depth, COL_GROUPS * cw), BF16),
            pltpu.VMEM((depth, COL_GROUPS * cw), BF16),
            pltpu.VMEM(first_down.shape, BF16),
            pltpu.VMEM(w_query.shape, BF16),
            pltpu.VMEM((pairs, length, 2 * LANES), BF16),
            pltpu.VMEM((pairs, 2 * LANES, length), BF16),
            pltpu.VMEM((pairs, length, 2 * LANES), BF16),
            pltpu.VMEM(w_out.shape, BF16),
            pltpu.VMEM((depth, COL_GROUPS * cw), BF16),
            pltpu.VMEM((depth, COL_GROUPS * cw), BF16),
            pltpu.VMEM(second_down.shape, BF16),
            pltpu.VMEM((n_tp,) + tokens.shape, BF16),
            *ffn_buffers,
            *tp_buffers,
            pltpu.VMEM((q_tiles, TILE, LANES), BF16),
            pltpu.VMEM((n_kv - 1, q_tiles, TILE, LANES), BF16),
            pltpu.VMEM((pairs, 2 * TILE, 2 * LANES), BF16),
            pltpu.VMEM((pairs, TILE, LANES), BF16),
            pltpu.VMEM((n_kv - 1, pairs, TILE, LANES), BF16),
            pltpu.VMEM((TILE, 2 * pairs), F32),
            pltpu.VMEM((n_kv - 1, TILE, 2 * pairs), F32),
            pltpu.VMEM((4 * pairs, pairs * LANES), BF16),
            pltpu.VMEM((pairs * TILE, LANES), F32),
            *tp_buffers,
            *ffn_buffers,
            pltpu.VMEM((n_tp, batch, own_width), BF16),
            pltpu.VMEM((n_tp - 1, batch, own_width), BF16),
            pltpu.SemaphoreType.DMA((6,)),
            pltpu.SemaphoreType.DMA((7 + kv_local * group,)),
            pltpu.SemaphoreType.DMA((8,)),
            pltpu.SemaphoreType.DMA((10,)),
            pltpu.SemaphoreType.DMA((3,)),
            pltpu.SemaphoreType.DMA((n_kv - 1,)),
            pltpu.SemaphoreType.DMA((n_kv - 1,)),
            pltpu.SemaphoreType.DMA((n_tp - 1,)),
            pltpu.SemaphoreType.DMA((n_tp - 1,)),
            pltpu.SemaphoreType.DMA((3,)),
            pltpu.SemaphoreType.DMA((3,)),
        ],
        compiler_params=pltpu.CompilerParams(
            collective_id=1, has_side_effects=True, vmem_limit_bytes=VMEM_LIMIT
        ),
    )(
        tokens, first_gain.reshape(1, -1), mix_gain.reshape(1, -1), second_gain.reshape(1, -1),
        map_weight.reshape(1, -1), head_gain.reshape(1, -1),
        first_gate, first_up, first_down, w_query, key_cache, value_cache, w_out,
        second_gate, second_up, second_down,
    )


def solution(mesh):
    placed = (
        P(None, ("kv", "tp")),
        P("kv"),
        P("kv", "tp"),
        P("kv", "tp"),
        P("tp", "kv"),
        P("kv"),
        P("kv", "tp"),
        P(None, "kv", "tp"),
        P(None, "kv", "tp"),
        P("tp"),
        P(),
        P("tp", "kv"),
        P("kv"),
        P("kv", "tp"),
        P("kv", "tp"),
        P("tp", "kv"),
    )
    return jax.shard_map(
        functools.partial(on_device, mesh.shape["kv"], mesh.shape["tp"]),
        mesh=mesh,
        in_specs=placed,
        out_specs=P(None, ("kv", "tp")),
        check_vma=False,
    )
```

```python
import functools
import math

import jax
import jax.numpy as jnp
from jax import lax
from jax.experimental import pallas as pl
from jax.experimental.pallas import tpu as pltpu
from jax.sharding import PartitionSpec as P

HEAD = 64
MAPS = 2
LANES = 128
TILE = 8
EPS = 1e-06
HEAD_SCALE = 0.8
SIDE = 4
STEPS = (2, 1, 3, 0)
ROW_GROUPS = 4
COL_GROUPS = 4
F32 = jnp.float32
BF16 = jnp.bfloat16
MESH = pl.DeviceIdType.MESH
VMEM_LIMIT = 60 * 1024 * 1024


def hops(d):
    return min(d, SIDE - d)


def kv_offsets():
    offs = [(a, b) for a in range(SIDE) for b in range(SIDE) if (a, b) != (0, 0)]
    return sorted(offs, key=lambda o: -(hops(o[0]) + hops(o[1])))


def tp_offsets():
    offs = [(a, b) for a in range(SIDE) for b in range(2) if (a, b) != (0, 0)]
    return sorted(offs, key=lambda o: -(2 * hops(o[0]) + o[1]))


def shifted(axis, offset):
    me = lax.axis_index(axis)
    inner = SIDE if axis == "kv" else 2
    high = lax.rem(me // inner + offset[0], SIDE)
    low = lax.rem(lax.rem(me, inner) + offset[1], inner)
    return high * inner + low


OFFSETS = {"kv": kv_offsets(), "tp": tp_offsets()}


def greet():
    barrier = pltpu.get_barrier_semaphore()
    total = 0
    for axis in ("kv", "tp"):
        for offset in OFFSETS[axis]:
            pl.semaphore_signal(
                barrier, inc=1, device_id={axis: shifted(axis, offset)}, device_id_type=MESH
            )
            total += 1
    pl.semaphore_wait(barrier, total)


def exchange(axis, source, target, send_sem, recv_sem):
    copies = []
    for k, offset in enumerate(OFFSETS[axis]):
        dest = shifted(axis, offset)
        copy = pltpu.make_async_remote_copy(
            src_ref=source(dest),
            dst_ref=target(k),
            send_sem=send_sem,
            recv_sem=recv_sem(k),
            device_id={axis: dest},
            device_id_type=MESH,
        )
        copy.start()
        copies.append(copy)
    return copies


def drain(axis, ref, sem):
    peer = shifted(axis, OFFSETS[axis][0])
    pltpu.make_async_remote_copy(
        src_ref=ref, dst_ref=ref, send_sem=sem, recv_sem=sem,
        device_id={axis: peer}, device_id_type=MESH,
    ).wait_recv()


def total_of(copies, own, recv):
    total = own
    for k in reversed(range(len(copies))):
        copies[k].wait_recv()
        total = total + recv[k].astype(F32)
    return total


def dot(a, b):
    return jnp.dot(a, b, preferred_element_type=F32)


def row_squares(h):
    return jnp.sum(h * h, axis=1, keepdims=True)


def squares_tile(h):
    s = row_squares(h)
    high = s.astype(BF16).astype(F32)
    lane = lax.broadcasted_iota(jnp.int32, (h.shape[0], LANES), 1)
    return jnp.where(lane < LANES // 2, high, s - high).astype(BF16)


def row_factor(tile, width):
    s = tile[:, :1] + tile[:, LANES // 2 : LANES // 2 + 1]
    return lax.rsqrt(s / width + EPS)


def feed_forward(n_kv, h, gain, w_gate, w_up, w_down, loads, scratch, sems, meanwhile):
    send, recv, act_own, act_all = scratch
    rs_send, rs_recv, ag_send, ag_recv = sems
    me = lax.axis_index("kv")
    hidden = w_down.shape[0]
    cw = act_own.shape[1]
    tile = squares_tile(h)
    scaled = (h * gain).astype(BF16)
    loads[0].wait()
    loads[1].wait()

    def product(c):
        columns = pl.ds(pl.multiple_of(c * cw, LANES), cw)
        return dot(scaled, jnp.concatenate([w_gate[:, columns], w_up[:, columns]], axis=1))

    z, y = me // SIDE, lax.rem(me, SIDE)
    groups = [lax.rem(y + step, SIDE) for step in STEPS]
    copies = [None] * len(OFFSETS["kv"])
    ahead = product(groups[0])
    for at, step in enumerate(STEPS):
        c, part = groups[at], ahead
        if at + 1 < len(STEPS):
            ahead = product(groups[at + 1])
        for r in range(ROW_GROUPS):
            rows = slice(r * TILE, (r + 1) * TILE)
            send[r * COL_GROUPS + c, :, : 2 * cw] = part[rows].astype(BF16)
            send[r * COL_GROUPS + c, :, 2 * cw :] = tile[rows]
        for up in STEPS:
            if (up, step) == (0, 0):
                continue
            k = OFFSETS["kv"].index((up, step))
            dest = lax.rem(z + up, SIDE) * SIDE + c
            copies[k] = pltpu.make_async_remote_copy(
                src_ref=send.at[dest], dst_ref=recv.at[k],
                send_sem=rs_send, recv_sem=rs_recv.at[k],
                device_id={"kv": dest}, device_id_type=MESH,
            )
            copies[k].start()
    total = total_of(copies, send[me].astype(F32), recv)
    factor = row_factor(total[:, 2 * cw :], h.shape[1] * n_kv)
    gate = total[:, :cw] * factor
    up = total[:, cw : 2 * cw] * factor
    act = (gate / (1.0 + jnp.exp(-gate)) * up).astype(BF16)
    act_own[...] = act
    act_all[me] = act
    exchange("kv", lambda d: act_own, lambda k: act_all.at[me], ag_send, lambda k: ag_recv)
    meanwhile()
    loads[2].wait()
    drain("kv", act_all.at[pl.ds(0, n_kv - 1)], ag_recv)
    out = None
    for c in range(COL_GROUPS):
        low = c * cw
        w = min(cw, hidden - low)
        block = jnp.concatenate(
            [act_all[r * COL_GROUPS + c, :, :w].astype(F32) for r in range(ROW_GROUPS)], axis=0
        ).astype(BF16)
        term = dot(block, w_down[low : low + w, :])
        out = term if out is None else out + term
    return out


def sum_over_tp(part, send, recv, send_sem, recv_sems, meanwhile=None):
    send[...] = part.astype(BF16)
    copies = exchange(
        "tp", lambda d: send, lambda k: recv.at[k], send_sem, lambda k: recv_sems.at[k]
    )
    if meanwhile is not None:
        meanwhile()
    return total_of(copies, send[...].astype(F32), recv)


def query_step(n_kv, h, gain, w_query, q_send, q_recv, send_sems, recv_sems):
    rows = h.shape[0]
    product = dot((h * gain).astype(BF16), w_query[...])
    row = lax.broadcasted_iota(jnp.int32, (rows, LANES), 0)
    lane = lax.broadcasted_iota(jnp.int32, (rows, LANES), 1)
    s = jnp.sum(jnp.where(row == lane, row_squares(h), 0.0), axis=0, keepdims=True)
    high = s.astype(BF16).astype(F32)
    first = lax.broadcasted_iota(jnp.int32, (TILE, LANES), 0)
    stats = jnp.where(first == 0, high, jnp.where(first == 1, s - high, 0.0))
    per = rows // TILE // 2
    count = 2 * per
    starts = (0, count + 1)
    spans = (pl.ds(0, count + 1), pl.ds(count + 1, count))
    for half in range(2):
        for r in range(per):
            for c in range(2):
                at = (half * per + r) * TILE
                q_send[starts[half] + 2 * r + c] = product[
                    at : at + TILE, c * LANES : (c + 1) * LANES
                ].astype(BF16)
    q_send[count] = stats.astype(BF16)
    rounds = [
        exchange(
            "kv", lambda d: q_send.at[spans[half]], lambda k: q_recv.at[k, spans[half]],
            send_sems[half], lambda k: recv_sems[half].at[k],
        )
        for half in range(2)
    ]

    def finish(half, factor):
        total = total_of(
            rounds[half], q_send[spans[half]].astype(F32), q_recv.at[:, spans[half]]
        )
        if half == 0:
            s = jnp.sum(total[count], axis=0, keepdims=True)
            factor = lax.rsqrt(s / (h.shape[1] * n_kv) + EPS)
            factor = jnp.sum(jnp.where(row == lane, factor, 0.0), axis=1, keepdims=True)
        mine = factor[half * per * TILE : (half + 1) * per * TILE]
        parts = [
            jnp.concatenate([total[2 * r + c] for r in range(per)], axis=0) * mine
            for c in range(2)
        ]
        low = lane[: per * TILE] < HEAD
        first_half = jnp.where(low, parts[0], pltpu.roll(parts[1], HEAD, 1))
        second_half = jnp.where(low, pltpu.roll(parts[0], HEAD, 1), parts[1])
        return (first_half.astype(BF16), second_half.astype(BF16)), factor

    return finish


def spread_queries(q_parts, qx, begin, count):
    batch = q_parts[0].shape[0]
    per = qx.shape[1]
    rows = count * per
    row = lax.broadcasted_iota(jnp.int32, (rows, batch), 0)
    col = lax.broadcasted_iota(jnp.int32, (rows, batch), 1)
    pick = jnp.where(col == row // per + count * lax.rem(row, 2), 1.0, 0.0).astype(BF16)
    wide_row = lax.broadcasted_iota(jnp.int32, (rows, LANES), 0)
    lane = lax.broadcasted_iota(jnp.int32, (rows, LANES), 1)
    which = lax.rem(wide_row // 2, 2)
    y = jnp.where(which == 0, dot(pick, q_parts[0]), dot(pick, q_parts[1]))
    mine = lane // (HEAD // MAPS) == lax.rem(wide_row // 4, 4)
    y = jnp.where(mine, y, 0.0)
    member = lax.rem(wide_row, 2)
    for i in range(2):
        block = jnp.where(member == i, y, 0.0).astype(BF16)
        qx[begin : begin + count, :, i * LANES : (i + 1) * LANES] = block.reshape(
            count, per, LANES
        )


def turn_keys(k_buf, k_turned, first, last):
    def body(p, carry):
        k_turned[p] = k_buf[p].T
        return carry

    lax.fori_loop(first, last, body, 0)


def attention_step(scale, qx, k_turned, v_buf, begin, end, o_send):
    row = lax.broadcasted_iota(jnp.int32, (2 * TILE, LANES), 0)
    lane = lax.broadcasted_iota(jnp.int32, (TILE, LANES), 1)
    first_member = lax.rem(row, 2) == 0
    low = lane < HEAD
    stats = jnp.zeros((TILE, LANES), F32)
    ahead = dot(qx[begin], k_turned[begin])
    for p in range(begin, end):
        s = ahead
        if p + 1 < end:
            ahead = dot(qx[p + 1], k_turned[p + 1])
        peak = jnp.max(s, axis=1, keepdims=True)
        e = jnp.exp2((s - peak) * scale)
        l = jnp.sum(e, axis=1, keepdims=True)
        lse = peak * scale + jnp.log2(l)
        stats = jnp.where(lane == 2 * (p - begin), lse[:TILE], stats)
        stats = jnp.where(lane == 2 * (p - begin) + 1, lse[TILE:], stats)
        o = dot(e.astype(BF16), v_buf[p]) / l
        o = jnp.where(first_member, o[:, :LANES], o[:, LANES:])
        o_send[p] = jnp.where(low, o[:TILE], o[TILE:]).astype(BF16)
    return stats


def split_three(x, width):
    high = x.astype(BF16).astype(F32)
    rest = x - high
    middle = rest.astype(BF16).astype(F32)
    low = rest - middle
    return (high + pltpu.roll(middle, width, 1) + pltpu.roll(low, 2 * width, 1)).astype(BF16)


def join_three(tile, width):
    x = tile.astype(F32)
    return x + pltpu.roll(x, LANES - width, 1) + pltpu.roll(x, LANES - 2 * width, 1)


def selector(sel):
    depth, width = sel.shape
    for j in range(width // LANES):
        row = lax.broadcasted_iota(jnp.int32, (depth, LANES), 0)
        lane = lax.broadcasted_iota(jnp.int32, (depth, LANES), 1)
        count = width // HEAD
        here = lax.rem(row, count) == 2 * j + lane // HEAD
        sel[:, j * LANES : (j + 1) * LANES] = jnp.where(here, 1.0, 0.0).astype(BF16)


def head_weights(map_weight, group, kv_local):
    row = lax.broadcasted_iota(jnp.int32, (TILE, LANES), 0)
    lane = lax.broadcasted_iota(jnp.int32, (TILE, LANES), 1)
    weight = jnp.zeros((TILE, LANES), F32)
    for k in range(kv_local):
        for g in range(group):
            here = (lax.rem(row // 2, group) == g) & (lane // HEAD == k)
            at = k * group + g
            weight = jnp.where(here, map_weight[:, at : at + 1], weight)
    return weight


def merge_heads(a, o_send, o_recv, st_send, st_recv, recv_sems, sel, weight, gain, heads):
    half = o_send.shape[0] // 2
    count = 2 * half
    others = st_recv.shape[0]
    lane = lax.broadcasted_iota(jnp.int32, (TILE, LANES), 1)
    drain("kv", st_recv.at[:, a], recv_sems.at[a])
    lses = [join_three(st_send[a], count)]
    lses += [join_three(st_recv[k, a], count) for k in range(others)]
    peak = functools.reduce(jnp.maximum, lses)
    weights = [jnp.exp2(lse - peak) for lse in lses]
    share = 1.0 / functools.reduce(jnp.add, weights)
    compact = jnp.concatenate([w * share for w in weights], axis=0)[:, :count]
    high = compact.astype(BF16)
    rest = (compact - high.astype(F32)).astype(BF16)
    spread = jnp.concatenate([high, rest], axis=1)
    drain("kv", o_recv.at[:, pl.ds(a * half, half)], recv_sems.at[2 + a])
    low = lane < HEAD
    for j in range(half // 2):
        wide = dot(spread, sel[:, 2 * j * LANES : 2 * (j + 1) * LANES])
        for i in range(2):
            p = a * half + 2 * j + i
            columns = slice(i * LANES, (i + 1) * LANES)
            outs = [o_send[p].astype(F32)] + [o_recv[k, p].astype(F32) for k in range(others)]
            merged = functools.reduce(
                jnp.add,
                [wide[d * TILE : (d + 1) * TILE, columns] * o for d, o in enumerate(outs)],
            )
            diff = merged - weight * pltpu.roll(merged, TILE // 2, 0)
            square = diff * diff
            left = jnp.sum(jnp.where(low, square, 0.0), axis=1, keepdims=True)
            right = jnp.sum(jnp.where(low, 0.0, square), axis=1, keepdims=True)
            mean = jnp.where(low, left, right) / HEAD
            heads[p * TILE : (p + 1) * TILE, :] = diff * lax.rsqrt(mean + EPS) * gain


def start_loads(pairs, sems):
    loads = [pltpu.make_async_copy(a, b, sems.at[i]) for i, (a, b) in enumerate(pairs)]
    for load in loads:
        load.start()
    return loads


def layer_kernel(
    n_kv, n_tp, kv_local, group, scale,
    tokens_any, gain1_any, gain_mix_any, gain2_any, weight_any, head_gain_any,
    gate1_any, up1_any, down1_any, query_any, key_any, value_any, out_any,
    gate2_any, up2_any, down2_any,
    mixed,
    tokens, first_gain, mix_gain, second_gain, map_weight, head_gain,
    w_gate1, w_up1, w_down1, w_query, k_buf, k_turned, v_buf, w_out, w_gate2, w_up2, w_down2,
    tok_all, rs1_send, rs1_recv, act1_own, act1_all, tp1_send, tp1_recv, q_send, q_recv, qx,
    o_send, o_recv, st_send, st_recv, sel, head_all, tp2_send, tp2_recv,
    rs2_send, rs2_recv, act2_own, act2_all, fin_send, fin_recv,
    small_sems, load_sems, cache_sems, send_sems, once_sems, kv_sems, second_sems, tp1_sems, tp2_sems, tp2_more_sems,
    o_send_sems, o_recv_sems,
):
    pairs = k_buf.shape[0]
    half = pairs // 2
    hidden = w_down1.shape[0]
    small = start_loads(
        (
            (tokens_any, tokens),
            (gain1_any, first_gain),
            (gain_mix_any, mix_gain),
            (gain2_any, second_gain),
            (weight_any, map_weight),
            (head_gain_any, head_gain),
        ),
        small_sems,
    )
    loads = start_loads(
        (
            (gate1_any, w_gate1.at[:, pl.ds(0, hidden)]),
            (up1_any, w_up1.at[:, pl.ds(0, hidden)]),
            (down1_any, w_down1),
            (query_any, w_query),
            (gate2_any, w_gate2.at[:, pl.ds(0, hidden)]),
            (up2_any, w_up2.at[:, pl.ds(0, hidden)]),
            (down2_any, w_down2),
        )
        + tuple(
            (
                out_any.at[pl.ds((k * group + g) * HEAD, HEAD)],
                w_out.at[pl.ds((g * kv_local + k) * HEAD, HEAD)],
            )
            for k in range(kv_local)
            for g in range(group)
        ),
        load_sems,
    )
    if hidden < w_gate1.shape[1]:
        for weight in (w_gate1, w_up1, w_gate2, w_up2):
            weight[:, hidden:] = jnp.zeros((weight.shape[0], weight.shape[1] - hidden), BF16)
    greet()
    cache_loads = start_loads(
        tuple(
            (cache.at[pl.ds((2 * a + i) * half, half)], buf.at[pl.ds(a * half, half), :, lanes])
            for cache, buf in ((key_any, k_buf), (value_any, v_buf))
            for a in range(2)
            for i, lanes in enumerate((pl.ds(0, LANES), pl.ds(LANES, LANES)))
        ),
        cache_sems,
    )
    for load in small:
        load.wait()
    tp = lax.axis_index("tp")
    tok_all[tp] = tokens[...]
    exchange(
        "tp", lambda d: tokens, lambda k: tok_all.at[tp], send_sems.at[0], lambda k: once_sems.at[0]
    )
    selector(sel)
    drain("tp", tok_all.at[pl.ds(0, n_tp - 1)], once_sems.at[0])
    h = jnp.concatenate([tok_all[j].astype(F32) for j in range(n_tp)], axis=1)

    def keys_first():
        cache_loads[0].wait()
        cache_loads[1].wait()
        turn_keys(k_buf, k_turned, 0, half)

    def keys_second():
        cache_loads[2].wait()
        cache_loads[3].wait()
        turn_keys(k_buf, k_turned, half, pairs)

    part = feed_forward(
        n_kv, h, first_gain[...], w_gate1, w_up1, w_down1, loads[:3],
        (rs1_send, rs1_recv, act1_own, act1_all),
        (send_sems.at[1], kv_sems, send_sems.at[2], once_sems.at[1]),
        keys_first,
    )
    h = h + 0.5 * sum_over_tp(part, tp1_send, tp1_recv, send_sems.at[3], tp1_sems, keys_second)
    loads[3].wait()
    finish = query_step(
        n_kv, h, mix_gain[...], w_query, q_send, q_recv,
        (send_sems.at[4], send_sems.at[9]), (kv_sems, second_sems),
    )
    factor = None
    for a in range(2):
        q_parts, factor = finish(a, factor)
        begin, end = a * half, (a + 1) * half
        spread_queries(q_parts, qx, begin, half)
        cache_loads[4 + 2 * a].wait()
        cache_loads[5 + 2 * a].wait()
        stats = attention_step(scale, qx, k_turned, v_buf, begin, end, o_send)
        st_send[a] = split_three(stats, 2 * half)
        exchange(
            "kv", lambda d: st_send.at[a], lambda k: st_recv.at[k, a],
            o_send_sems.at[a], lambda k: o_recv_sems.at[a],
        )
        span = pl.ds(begin, half)
        exchange(
            "kv", lambda d: o_send.at[span], lambda k: o_recv.at[k, span],
            o_send_sems.at[2 + a], lambda k: o_recv_sems.at[2 + a],
        )
    weight = head_weights(map_weight, group, kv_local)
    gain = jnp.concatenate([head_gain[...] * HEAD_SCALE] * kv_local, axis=1)
    for load in loads[7:]:
        load.wait()
    rounds = []
    for a in range(2):
        merge_heads(a, o_send, o_recv, st_send, st_recv, o_recv_sems, sel, weight, gain, head_all)
        heads = jnp.concatenate(
            [
                jnp.concatenate(
                    [
                        head_all[pl.ds(a * half * TILE + 2 * g + i, half, stride=TILE), :]
                        for g in range(group)
                    ],
                    axis=1,
                )
                for i in range(2)
            ],
            axis=0,
        ).astype(BF16)
        span = pl.ds(2 * a * half, 2 * half)
        tp2_send[span, :] = dot(heads, w_out[...]).astype(BF16)
        sems = (tp2_sems, tp2_more_sems)[a]
        rounds.append(
            exchange(
                "tp", lambda d: tp2_send.at[span], lambda k: tp2_recv.at[k, span],
                send_sems.at[5 * (a + 1)], lambda k: sems.at[k],
            )
        )
    sums = []
    for a in range(2):
        span = pl.ds(2 * a * half, 2 * half)
        sums.append(total_of(rounds[a], tp2_send[span, :].astype(F32), tp2_recv.at[:, span]))
    h = h + jnp.concatenate(sums, axis=0)
    part = feed_forward(
        n_kv, h, second_gain[...], w_gate2, w_up2, w_down2, loads[4:7],
        (rs2_send, rs2_recv, act2_own, act2_all),
        (send_sems.at[6], kv_sems, send_sems.at[7], once_sems.at[2]),
        lambda: None,
    )
    batch, width = mixed.shape
    own = jnp.zeros((batch, width), F32)
    for j in range(n_tp):
        columns = slice(j * width, (j + 1) * width)
        fin_send[j] = part[:, columns].astype(BF16)
        own = jnp.where(tp == j, h[:, columns], own)
    copies = exchange(
        "tp", lambda d: fin_send.at[d], lambda k: fin_recv.at[k],
        send_sems.at[8], lambda k: tp1_sems.at[k],
    )
    drain("tp", tok_all.at[pl.ds(0, n_tp - 1)], send_sems.at[0])
    drain("kv", rs1_recv, send_sems.at[1])
    drain("kv", act1_all.at[pl.ds(0, n_kv - 1)], send_sems.at[2])
    drain("tp", tp1_recv, send_sems.at[3])
    split = q_recv.shape[1] // 2 + 1
    drain("kv", q_recv.at[:, pl.ds(0, split)], send_sems.at[4])
    drain("kv", q_recv.at[:, pl.ds(split, split - 1)], send_sems.at[9])
    for a in range(2):
        drain("kv", st_recv.at[:, a], o_send_sems.at[a])
        drain("kv", o_recv.at[:, pl.ds(a * half, half)], o_send_sems.at[2 + a])
        drain("tp", tp2_recv.at[:, pl.ds(2 * a * half, 2 * half)], send_sems.at[5 * (a + 1)])
    drain("kv", rs2_recv, send_sems.at[6])
    drain("kv", act2_all.at[pl.ds(0, n_kv - 1)], send_sems.at[7])
    total = total_of(copies, fin_send[tp].astype(F32), fin_recv)
    drain("tp", fin_recv, send_sems.at[8])
    mixed[...] = (own + 0.5 * total).astype(BF16)


def on_device(
    n_kv, n_tp, tokens, first_gain, first_gate, first_up, first_down, mix_gain, w_query,
    key_cache, value_cache, map_weight, head_gain, w_out, second_gain, second_gate, second_up,
    second_down,
):
    batch, own_width = tokens.shape
    depth, hidden = first_gate.shape
    length = key_cache.shape[1]
    columns = w_query.shape[1]
    kv_local = key_cache.shape[2] // HEAD
    group = columns // (kv_local * HEAD)
    pairs = batch // 2
    cw = -(-hidden // (LANES * COL_GROUPS)) * LANES
    hbm = pl.BlockSpec(memory_space=pl.ANY)
    ffn_buffers = [
        pltpu.VMEM((n_kv, TILE, 2 * cw + LANES), BF16),
        pltpu.VMEM((n_kv - 1, TILE, 2 * cw + LANES), BF16),
        pltpu.VMEM((TILE, cw), BF16),
        pltpu.VMEM((n_kv, TILE, cw), BF16),
    ]
    tp_buffers = [pltpu.VMEM((batch, depth), BF16), pltpu.VMEM((n_tp - 1, batch, depth), BF16)]
    q_tiles = 2 * (batch // TILE) + 1
    return pl.pallas_call(
        functools.partial(
            layer_kernel, n_kv, n_tp, kv_local, group, math.log2(math.e) / math.sqrt(HEAD // MAPS)
        ),
        out_shape=pltpu.VMEM((batch, depth // n_tp), BF16),
        in_specs=[hbm] * 16,
        out_specs=pl.BlockSpec(memory_space=pltpu.VMEM),
        scratch_shapes=[
            pltpu.VMEM(tokens.shape, BF16),
            pltpu.VMEM((1, depth), F32),
            pltpu.VMEM((1, depth), F32),
            pltpu.VMEM((1, depth), F32),
            pltpu.VMEM((1, kv_local * group), F32),
            pltpu.VMEM((1, HEAD), F32),
            pltpu.VMEM((depth, COL_GROUPS * cw), BF16),
            pltpu.VMEM((depth, COL_GROUPS * cw), BF16),
            pltpu.VMEM(first_down.shape, BF16),
            pltpu.VMEM(w_query.shape, BF16),
            pltpu.VMEM((pairs, length, 2 * LANES), BF16),
            pltpu.VMEM((pairs, 2 * LANES, length), BF16),
            pltpu.VMEM((pairs, length, 2 * LANES), BF16),
            pltpu.VMEM(w_out.shape, BF16),
            pltpu.VMEM((depth, COL_GROUPS * cw), BF16),
            pltpu.VMEM((depth, COL_GROUPS * cw), BF16),
            pltpu.VMEM(second_down.shape, BF16),
            pltpu.VMEM((n_tp,) + tokens.shape, BF16),
            *ffn_buffers,
            *tp_buffers,
            pltpu.VMEM((q_tiles, TILE, LANES), BF16),
            pltpu.VMEM((n_kv - 1, q_tiles, TILE, LANES), BF16),
            pltpu.VMEM((pairs, 2 * TILE, 2 * LANES), BF16),
            pltpu.VMEM((pairs, TILE, LANES), BF16),
            pltpu.VMEM((n_kv - 1, pairs, TILE, LANES), BF16),
            pltpu.VMEM((2, TILE, LANES), BF16),
            pltpu.VMEM((n_kv - 1, 2, TILE, LANES), BF16),
            pltpu.VMEM((2 * pairs, pairs // 2 * LANES), BF16),
            pltpu.VMEM((pairs * TILE, LANES), F32),
            *tp_buffers,
            *ffn_buffers,
            pltpu.VMEM((n_tp, batch, own_width), BF16),
            pltpu.VMEM((n_tp - 1, batch, own_width), BF16),
            pltpu.SemaphoreType.DMA((6,)),
            pltpu.SemaphoreType.DMA((7 + kv_local * group,)),
            pltpu.SemaphoreType.DMA((8,)),
            pltpu.SemaphoreType.DMA((11,)),
            pltpu.SemaphoreType.DMA((3,)),
            pltpu.SemaphoreType.DMA((n_kv - 1,)),
            pltpu.SemaphoreType.DMA((n_kv - 1,)),
            pltpu.SemaphoreType.DMA((n_tp - 1,)),
            pltpu.SemaphoreType.DMA((n_tp - 1,)),
            pltpu.SemaphoreType.DMA((n_tp - 1,)),
            pltpu.SemaphoreType.DMA((4,)),
            pltpu.SemaphoreType.DMA((4,)),
        ],
        compiler_params=pltpu.CompilerParams(
            collective_id=1, has_side_effects=True, vmem_limit_bytes=VMEM_LIMIT
        ),
    )(
        tokens, first_gain.reshape(1, -1), mix_gain.reshape(1, -1), second_gain.reshape(1, -1),
        map_weight.reshape(1, -1), head_gain.reshape(1, -1),
        first_gate, first_up, first_down, w_query, key_cache, value_cache, w_out,
        second_gate, second_up, second_down,
    )


def solution(mesh):
    placed = (
        P(None, ("kv", "tp")),
        P("kv"),
        P("kv", "tp"),
        P("kv", "tp"),
        P("tp", "kv"),
        P("kv"),
        P("kv", "tp"),
        P(None, "kv", "tp"),
        P(None, "kv", "tp"),
        P("tp"),
        P(),
        P("tp", "kv"),
        P("kv"),
        P("kv", "tp"),
        P("kv", "tp"),
        P("tp", "kv"),
    )
    return jax.shard_map(
        functools.partial(on_device, mesh.shape["kv"], mesh.shape["tp"]),
        mesh=mesh,
        in_specs=placed,
        out_specs=P(None, ("kv", "tp")),
        check_vma=False,
    )
```

```python
import functools
import math

import jax
import jax.numpy as jnp
from jax import lax
from jax.experimental import pallas as pl
from jax.experimental.pallas import tpu as pltpu
from jax.sharding import PartitionSpec as P

HEAD = 64
MAPS = 2
LANES = 128
TILE = 8
EPS = 1e-06
HEAD_SCALE = 0.8
SIDE = 4
STEPS = (2, 1, 3, 0)
ROW_GROUPS = 4
COL_GROUPS = 4
F32 = jnp.float32
BF16 = jnp.bfloat16
MESH = pl.DeviceIdType.MESH
VMEM_LIMIT = 60 * 1024 * 1024


def hops(d):
    return min(d, SIDE - d)


def kv_offsets():
    offs = [(a, b) for a in range(SIDE) for b in range(SIDE) if (a, b) != (0, 0)]
    return sorted(offs, key=lambda o: -(hops(o[0]) + hops(o[1])))


def tp_offsets():
    offs = [(a, b) for a in range(SIDE) for b in range(2) if (a, b) != (0, 0)]
    return sorted(offs, key=lambda o: -(2 * hops(o[0]) + o[1]))


def shifted(axis, offset):
    me = lax.axis_index(axis)
    inner = SIDE if axis == "kv" else 2
    high = lax.rem(me // inner + offset[0], SIDE)
    low = lax.rem(lax.rem(me, inner) + offset[1], inner)
    return high * inner + low


OFFSETS = {"kv": kv_offsets(), "tp": tp_offsets()}


def greet():
    barrier = pltpu.get_barrier_semaphore()
    total = 0
    for axis in ("kv", "tp"):
        for offset in OFFSETS[axis]:
            pl.semaphore_signal(
                barrier, inc=1, device_id={axis: shifted(axis, offset)}, device_id_type=MESH
            )
            total += 1
    pl.semaphore_wait(barrier, total)


def exchange(axis, source, target, send_sem, recv_sem):
    copies = []
    for k, offset in enumerate(OFFSETS[axis]):
        dest = shifted(axis, offset)
        copy = pltpu.make_async_remote_copy(
            src_ref=source(dest),
            dst_ref=target(k),
            send_sem=send_sem,
            recv_sem=recv_sem(k),
            device_id={axis: dest},
            device_id_type=MESH,
        )
        copy.start()
        copies.append(copy)
    return copies


def drain(axis, ref, sem):
    peer = shifted(axis, OFFSETS[axis][0])
    pltpu.make_async_remote_copy(
        src_ref=ref, dst_ref=ref, send_sem=sem, recv_sem=sem,
        device_id={axis: peer}, device_id_type=MESH,
    ).wait_recv()


def total_of(copies, own, recv):
    total = own
    for k in reversed(range(len(copies))):
        copies[k].wait_recv()
        total = total + recv[k].astype(F32)
    return total


def dot(a, b):
    return jnp.dot(a, b, preferred_element_type=F32)


def row_squares(h):
    return jnp.sum(h * h, axis=1, keepdims=True)


def squares_tile(h):
    s = row_squares(h)
    high = s.astype(BF16).astype(F32)
    lane = lax.broadcasted_iota(jnp.int32, (h.shape[0], LANES), 1)
    return jnp.where(lane < LANES // 2, high, s - high).astype(BF16)


def row_factor(tile, width):
    s = tile[:, :1] + tile[:, LANES // 2 : LANES // 2 + 1]
    return lax.rsqrt(s / width + EPS)


def feed_forward(n_kv, h, gain, w_gate, w_up, w_down, loads, scratch, sems, meanwhile):
    send, recv, act_own, act_all = scratch
    rs_send, rs_recv, ag_send, ag_recv = sems
    me = lax.axis_index("kv")
    hidden = w_down.shape[0]
    cw = act_own.shape[1]
    tile = squares_tile(h)
    scaled = (h * gain).astype(BF16)
    loads[0].wait()
    loads[1].wait()

    def product(c):
        columns = pl.ds(pl.multiple_of(c * cw, LANES), cw)
        return dot(scaled, jnp.concatenate([w_gate[:, columns], w_up[:, columns]], axis=1))

    z, y = me // SIDE, lax.rem(me, SIDE)
    groups = [lax.rem(y + step, SIDE) for step in STEPS]
    copies = [None] * len(OFFSETS["kv"])
    ahead = product(groups[0])
    for at, step in enumerate(STEPS):
        c, part = groups[at], ahead
        if at + 1 < len(STEPS):
            ahead = product(groups[at + 1])
        for r in range(ROW_GROUPS):
            rows = slice(r * TILE, (r + 1) * TILE)
            send[r * COL_GROUPS + c, :, : 2 * cw] = part[rows].astype(BF16)
            send[r * COL_GROUPS + c, :, 2 * cw :] = tile[rows]
        for up in STEPS:
            if (up, step) == (0, 0):
                continue
            k = OFFSETS["kv"].index((up, step))
            dest = lax.rem(z + up, SIDE) * SIDE + c
            copies[k] = pltpu.make_async_remote_copy(
                src_ref=send.at[dest], dst_ref=recv.at[k],
                send_sem=rs_send, recv_sem=rs_recv.at[k],
                device_id={"kv": dest}, device_id_type=MESH,
            )
            copies[k].start()
    total = total_of(copies, send[me].astype(F32), recv)
    factor = row_factor(total[:, 2 * cw :], h.shape[1] * n_kv)
    gate = total[:, :cw] * factor
    up = total[:, cw : 2 * cw] * factor
    act = (gate / (1.0 + jnp.exp(-gate)) * up).astype(BF16)
    act_own[...] = act
    act_all[me] = act
    exchange("kv", lambda d: act_own, lambda k: act_all.at[me], ag_send, lambda k: ag_recv)
    meanwhile()
    loads[2].wait()
    drain("kv", act_all.at[pl.ds(0, n_kv - 1)], ag_recv)
    out = None
    for c in range(COL_GROUPS):
        low = c * cw
        w = min(cw, hidden - low)
        block = jnp.concatenate(
            [act_all[r * COL_GROUPS + c, :, :w].astype(F32) for r in range(ROW_GROUPS)], axis=0
        ).astype(BF16)
        term = dot(block, w_down[low : low + w, :])
        out = term if out is None else out + term
    return out


def sum_over_tp(part, send, recv, send_sem, recv_sems, meanwhile=None):
    send[...] = part.astype(BF16)
    copies = exchange(
        "tp", lambda d: send, lambda k: recv.at[k], send_sem, lambda k: recv_sems.at[k]
    )
    if meanwhile is not None:
        meanwhile()
    return total_of(copies, send[...].astype(F32), recv)


def query_step(n_kv, h, gain, w_query, q_send, q_recv, send_sems, recv_sems):
    rows = h.shape[0]
    product = dot((h * gain).astype(BF16), w_query[...])
    row = lax.broadcasted_iota(jnp.int32, (rows, LANES), 0)
    lane = lax.broadcasted_iota(jnp.int32, (rows, LANES), 1)
    s = jnp.sum(jnp.where(row == lane, row_squares(h), 0.0), axis=0, keepdims=True)
    high = s.astype(BF16).astype(F32)
    first = lax.broadcasted_iota(jnp.int32, (TILE, LANES), 0)
    stats = jnp.where(first == 0, high, jnp.where(first == 1, s - high, 0.0))
    per = rows // TILE // 2
    count = 2 * per
    starts = (0, count + 1)
    spans = (pl.ds(0, count + 1), pl.ds(count + 1, count))
    for half in range(2):
        for r in range(per):
            for c in range(2):
                at = (half * per + r) * TILE
                q_send[starts[half] + 2 * r + c] = product[
                    at : at + TILE, c * LANES : (c + 1) * LANES
                ].astype(BF16)
    q_send[count] = stats.astype(BF16)
    rounds = [
        exchange(
            "kv", lambda d: q_send.at[spans[half]], lambda k: q_recv.at[k, spans[half]],
            send_sems[half], lambda k: recv_sems[half].at[k],
        )
        for half in range(2)
    ]

    def finish(half, factor):
        total = total_of(
            rounds[half], q_send[spans[half]].astype(F32), q_recv.at[:, spans[half]]
        )
        if half == 0:
            s = jnp.sum(total[count], axis=0, keepdims=True)
            factor = lax.rsqrt(s / (h.shape[1] * n_kv) + EPS)
            factor = jnp.sum(jnp.where(row == lane, factor, 0.0), axis=1, keepdims=True)
        mine = factor[half * per * TILE : (half + 1) * per * TILE]
        parts = [
            jnp.concatenate([total[2 * r + c] for r in range(per)], axis=0) * mine
            for c in range(2)
        ]
        low = lane[: per * TILE] < HEAD
        first_half = jnp.where(low, parts[0], pltpu.roll(parts[1], HEAD, 1))
        second_half = jnp.where(low, pltpu.roll(parts[0], HEAD, 1), parts[1])
        return (first_half.astype(BF16), second_half.astype(BF16)), factor

    return finish


def spread_queries(q_parts, qx, begin, count):
    batch = q_parts[0].shape[0]
    per = qx.shape[1]
    rows = count * per
    row = lax.broadcasted_iota(jnp.int32, (rows, batch), 0)
    col = lax.broadcasted_iota(jnp.int32, (rows, batch), 1)
    pick = jnp.where(col == row // per + count * lax.rem(row, 2), 1.0, 0.0).astype(BF16)
    wide_row = lax.broadcasted_iota(jnp.int32, (rows, LANES), 0)
    lane = lax.broadcasted_iota(jnp.int32, (rows, LANES), 1)
    which = lax.rem(wide_row // 2, 2)
    y = jnp.where(which == 0, dot(pick, q_parts[0]), dot(pick, q_parts[1]))
    mine = lane // (HEAD // MAPS) == lax.rem(wide_row // 4, 4)
    y = jnp.where(mine, y, 0.0)
    member = lax.rem(wide_row, 2)
    for i in range(2):
        block = jnp.where(member == i, y, 0.0).astype(BF16)
        qx[begin : begin + count, :, i * LANES : (i + 1) * LANES] = block.reshape(
            count, per, LANES
        )


def turn_keys(k_buf, k_turned, first, last):
    def body(p, carry):
        k_turned[p] = k_buf[p].T
        return carry

    lax.fori_loop(first, last, body, 0)


def attention_step(scale, qx, k_turned, v_buf, begin, end, o_send):
    row = lax.broadcasted_iota(jnp.int32, (2 * TILE, LANES), 0)
    lane = lax.broadcasted_iota(jnp.int32, (TILE, LANES), 1)
    first_member = lax.rem(row, 2) == 0
    low = lane < HEAD
    stats = jnp.zeros((TILE, LANES), F32)
    ahead = dot(qx[begin], k_turned[begin])
    for p in range(begin, end):
        s = ahead
        if p + 1 < end:
            ahead = dot(qx[p + 1], k_turned[p + 1])
        peak = jnp.max(s, axis=1, keepdims=True)
        e = jnp.exp2((s - peak) * scale)
        l = jnp.sum(e, axis=1, keepdims=True)
        lse = peak * scale + jnp.log2(l)
        stats = jnp.where(lane == 2 * (p - begin), lse[:TILE], stats)
        stats = jnp.where(lane == 2 * (p - begin) + 1, lse[TILE:], stats)
        o = dot(e.astype(BF16), v_buf[p]) / l
        o = jnp.where(first_member, o[:, :LANES], o[:, LANES:])
        o_send[p] = jnp.where(low, o[:TILE], o[TILE:]).astype(BF16)
    return stats


def split_three(x, width):
    high = x.astype(BF16).astype(F32)
    rest = x - high
    middle = rest.astype(BF16).astype(F32)
    low = rest - middle
    return (high + pltpu.roll(middle, width, 1) + pltpu.roll(low, 2 * width, 1)).astype(BF16)


def join_three(tile, width):
    x = tile.astype(F32)
    return x + pltpu.roll(x, LANES - width, 1) + pltpu.roll(x, LANES - 2 * width, 1)


def selector(sel):
    depth, width = sel.shape
    for j in range(width // LANES):
        row = lax.broadcasted_iota(jnp.int32, (depth, LANES), 0)
        lane = lax.broadcasted_iota(jnp.int32, (depth, LANES), 1)
        count = width // HEAD
        here = lax.rem(row, count) == 2 * j + lane // HEAD
        sel[:, j * LANES : (j + 1) * LANES] = jnp.where(here, 1.0, 0.0).astype(BF16)


def head_weights(map_weight, group, kv_local):
    row = lax.broadcasted_iota(jnp.int32, (TILE, LANES), 0)
    lane = lax.broadcasted_iota(jnp.int32, (TILE, LANES), 1)
    weight = jnp.zeros((TILE, LANES), F32)
    for k in range(kv_local):
        for g in range(group):
            here = (lax.rem(row // 2, group) == g) & (lane // HEAD == k)
            at = k * group + g
            weight = jnp.where(here, map_weight[:, at : at + 1], weight)
    return weight


def merge_heads(a, o_send, o_recv, st_send, st_recv, recv_sems, sel, weight, gain, heads):
    half = o_send.shape[0] // 2
    count = 2 * half
    others = st_recv.shape[0]
    lane = lax.broadcasted_iota(jnp.int32, (TILE, LANES), 1)
    drain("kv", st_recv.at[:, a], recv_sems.at[a])
    lses = [join_three(st_send[a], count)]
    lses += [join_three(st_recv[k, a], count) for k in range(others)]
    peak = functools.reduce(jnp.maximum, lses)
    weights = [jnp.exp2(lse - peak) for lse in lses]
    share = 1.0 / functools.reduce(jnp.add, weights)
    compact = jnp.concatenate([w * share for w in weights], axis=0)[:, :count]
    high = compact.astype(BF16)
    rest = (compact - high.astype(F32)).astype(BF16)
    spread = jnp.concatenate([high, rest], axis=1)
    drain("kv", o_recv.at[:, pl.ds(a * half, half)], recv_sems.at[2 + a])
    low = lane < HEAD
    for j in range(half // 2):
        wide = dot(spread, sel[:, 2 * j * LANES : 2 * (j + 1) * LANES])
        for i in range(2):
            p = a * half + 2 * j + i
            columns = slice(i * LANES, (i + 1) * LANES)
            outs = [o_send[p].astype(F32)] + [o_recv[k, p].astype(F32) for k in range(others)]
            merged = functools.reduce(
                jnp.add,
                [wide[d * TILE : (d + 1) * TILE, columns] * o for d, o in enumerate(outs)],
            )
            diff = merged - weight * pltpu.roll(merged, TILE // 2, 0)
            square = diff * diff
            left = jnp.sum(jnp.where(low, square, 0.0), axis=1, keepdims=True)
            right = jnp.sum(jnp.where(low, 0.0, square), axis=1, keepdims=True)
            mean = jnp.where(low, left, right) / HEAD
            heads[p * TILE : (p + 1) * TILE, :] = diff * lax.rsqrt(mean + EPS) * gain


def start_loads(pairs, sems):
    loads = [pltpu.make_async_copy(a, b, sems.at[i]) for i, (a, b) in enumerate(pairs)]
    for load in loads:
        load.start()
    return loads


def layer_kernel(
    n_kv, n_tp, kv_local, group, scale,
    tokens_any, gain1_any, gain_mix_any, gain2_any, weight_any, head_gain_any,
    gate1_any, up1_any, down1_any, query_any, key_any, value_any, out_any,
    gate2_any, up2_any, down2_any,
    mixed,
    tokens, first_gain, mix_gain, second_gain, map_weight, head_gain,
    w_gate1, w_up1, w_down1, w_query, k_buf, k_turned, v_buf, w_out, w_gate2, w_up2, w_down2,
    tok_all, rs1_send, rs1_recv, act1_own, act1_all, tp1_send, tp1_recv, q_send, q_recv, qx,
    o_send, o_recv, st_send, st_recv, sel, head_all, tp2_send, tp2_recv,
    rs2_send, rs2_recv, act2_own, act2_all, fin_send, fin_recv,
    small_sems, load_sems, cache_sems, send_sems, once_sems, kv_sems, second_sems, tp1_sems, tp2_sems, tp2_more_sems,
    o_send_sems, o_recv_sems,
):
    pairs = k_buf.shape[0]
    half = pairs // 2
    hidden = w_down1.shape[0]
    small = start_loads(
        (
            (tokens_any, tokens),
            (gain1_any, first_gain),
            (gain_mix_any, mix_gain),
            (gain2_any, second_gain),
            (weight_any, map_weight),
            (head_gain_any, head_gain),
        ),
        small_sems,
    )
    loads = start_loads(
        (
            (gate1_any, w_gate1.at[:, pl.ds(0, hidden)]),
            (up1_any, w_up1.at[:, pl.ds(0, hidden)]),
            (down1_any, w_down1),
            (query_any, w_query),
            (gate2_any, w_gate2.at[:, pl.ds(0, hidden)]),
            (up2_any, w_up2.at[:, pl.ds(0, hidden)]),
            (down2_any, w_down2),
        )
        + tuple(
            (
                out_any.at[pl.ds((k * group + g) * HEAD, HEAD)],
                w_out.at[pl.ds((g * kv_local + k) * HEAD, HEAD)],
            )
            for k in range(kv_local)
            for g in range(group)
        ),
        load_sems,
    )
    if hidden < w_gate1.shape[1]:
        for weight in (w_gate1, w_up1, w_gate2, w_up2):
            weight[:, hidden:] = jnp.zeros((weight.shape[0], weight.shape[1] - hidden), BF16)
    greet()
    for load in small:
        load.wait()
    tp = lax.axis_index("tp")
    tok_all[tp] = tokens[...]
    exchange(
        "tp", lambda d: tokens, lambda k: tok_all.at[tp], send_sems.at[0], lambda k: once_sems.at[0]
    )
    cache_loads = start_loads(
        tuple(
            (cache.at[pl.ds((2 * a + i) * half, half)], buf.at[pl.ds(a * half, half), :, lanes])
            for cache, buf in ((key_any, k_buf), (value_any, v_buf))
            for a in range(2)
            for i, lanes in enumerate((pl.ds(0, LANES), pl.ds(LANES, LANES)))
        ),
        cache_sems,
    )
    selector(sel)
    drain("tp", tok_all.at[pl.ds(0, n_tp - 1)], once_sems.at[0])
    h = jnp.concatenate([tok_all[j].astype(F32) for j in range(n_tp)], axis=1)

    def keys_first():
        cache_loads[0].wait()
        cache_loads[1].wait()
        turn_keys(k_buf, k_turned, 0, half)

    def keys_second():
        cache_loads[2].wait()
        cache_loads[3].wait()
        turn_keys(k_buf, k_turned, half, pairs)

    part = feed_forward(
        n_kv, h, first_gain[...], w_gate1, w_up1, w_down1, loads[:3],
        (rs1_send, rs1_recv, act1_own, act1_all),
        (send_sems.at[1], kv_sems, send_sems.at[2], once_sems.at[1]),
        keys_first,
    )
    h = h + 0.5 * sum_over_tp(part, tp1_send, tp1_recv, send_sems.at[3], tp1_sems, keys_second)
    loads[3].wait()
    finish = query_step(
        n_kv, h, mix_gain[...], w_query, q_send, q_recv,
        (send_sems.at[4], send_sems.at[9]), (kv_sems, second_sems),
    )
    factor = None
    for a in range(2):
        q_parts, factor = finish(a, factor)
        begin, end = a * half, (a + 1) * half
        spread_queries(q_parts, qx, begin, half)
        cache_loads[4 + 2 * a].wait()
        cache_loads[5 + 2 * a].wait()
        stats = attention_step(scale, qx, k_turned, v_buf, begin, end, o_send)
        st_send[a] = split_three(stats, 2 * half)
        exchange(
            "kv", lambda d: st_send.at[a], lambda k: st_recv.at[k, a],
            o_send_sems.at[a], lambda k: o_recv_sems.at[a],
        )
        span = pl.ds(begin, half)
        exchange(
            "kv", lambda d: o_send.at[span], lambda k: o_recv.at[k, span],
            o_send_sems.at[2 + a], lambda k: o_recv_sems.at[2 + a],
        )
    weight = head_weights(map_weight, group, kv_local)
    gain = jnp.concatenate([head_gain[...] * HEAD_SCALE] * kv_local, axis=1)
    for load in loads[7:]:
        load.wait()
    rounds = []
    for a in range(2):
        merge_heads(a, o_send, o_recv, st_send, st_recv, o_recv_sems, sel, weight, gain, head_all)
        heads = jnp.concatenate(
            [
                jnp.concatenate(
                    [
                        head_all[pl.ds(a * half * TILE + 2 * g + i, half, stride=TILE), :]
                        for g in range(group)
                    ],
                    axis=1,
                )
                for i in range(2)
            ],
            axis=0,
        ).astype(BF16)
        span = pl.ds(2 * a * half, 2 * half)
        tp2_send[span, :] = dot(heads, w_out[...]).astype(BF16)
        sems = (tp2_sems, tp2_more_sems)[a]
        rounds.append(
            exchange(
                "tp", lambda d: tp2_send.at[span], lambda k: tp2_recv.at[k, span],
                send_sems.at[5 * (a + 1)], lambda k: sems.at[k],
            )
        )
    sums = []
    for a in range(2):
        span = pl.ds(2 * a * half, 2 * half)
        sums.append(total_of(rounds[a], tp2_send[span, :].astype(F32), tp2_recv.at[:, span]))
    h = h + jnp.concatenate(sums, axis=0)
    part = feed_forward(
        n_kv, h, second_gain[...], w_gate2, w_up2, w_down2, loads[4:7],
        (rs2_send, rs2_recv, act2_own, act2_all),
        (send_sems.at[6], kv_sems, send_sems.at[7], once_sems.at[2]),
        lambda: None,
    )
    batch, width = mixed.shape
    own = jnp.zeros((batch, width), F32)
    for j in range(n_tp):
        columns = slice(j * width, (j + 1) * width)
        fin_send[j] = part[:, columns].astype(BF16)
        own = jnp.where(tp == j, h[:, columns], own)
    copies = exchange(
        "tp", lambda d: fin_send.at[d], lambda k: fin_recv.at[k],
        send_sems.at[8], lambda k: tp1_sems.at[k],
    )
    drain("tp", tok_all.at[pl.ds(0, n_tp - 1)], send_sems.at[0])
    drain("kv", rs1_recv, send_sems.at[1])
    drain("kv", act1_all.at[pl.ds(0, n_kv - 1)], send_sems.at[2])
    drain("tp", tp1_recv, send_sems.at[3])
    split = q_recv.shape[1] // 2 + 1
    drain("kv", q_recv.at[:, pl.ds(0, split)], send_sems.at[4])
    drain("kv", q_recv.at[:, pl.ds(split, split - 1)], send_sems.at[9])
    for a in range(2):
        drain("kv", st_recv.at[:, a], o_send_sems.at[a])
        drain("kv", o_recv.at[:, pl.ds(a * half, half)], o_send_sems.at[2 + a])
        drain("tp", tp2_recv.at[:, pl.ds(2 * a * half, 2 * half)], send_sems.at[5 * (a + 1)])
    drain("kv", rs2_recv, send_sems.at[6])
    drain("kv", act2_all.at[pl.ds(0, n_kv - 1)], send_sems.at[7])
    total = total_of(copies, fin_send[tp].astype(F32), fin_recv)
    drain("tp", fin_recv, send_sems.at[8])
    mixed[...] = (own + 0.5 * total).astype(BF16)


def on_device(
    n_kv, n_tp, tokens, first_gain, first_gate, first_up, first_down, mix_gain, w_query,
    key_cache, value_cache, map_weight, head_gain, w_out, second_gain, second_gate, second_up,
    second_down,
):
    batch, own_width = tokens.shape
    depth, hidden = first_gate.shape
    length = key_cache.shape[1]
    columns = w_query.shape[1]
    kv_local = key_cache.shape[2] // HEAD
    group = columns // (kv_local * HEAD)
    pairs = batch // 2
    cw = -(-hidden // (LANES * COL_GROUPS)) * LANES
    hbm = pl.BlockSpec(memory_space=pl.ANY)
    ffn_buffers = [
        pltpu.VMEM((n_kv, TILE, 2 * cw + LANES), BF16),
        pltpu.VMEM((n_kv - 1, TILE, 2 * cw + LANES), BF16),
        pltpu.VMEM((TILE, cw), BF16),
        pltpu.VMEM((n_kv, TILE, cw), BF16),
    ]
    tp_buffers = [pltpu.VMEM((batch, depth), BF16), pltpu.VMEM((n_tp - 1, batch, depth), BF16)]
    q_tiles = 2 * (batch // TILE) + 1
    return pl.pallas_call(
        functools.partial(
            layer_kernel, n_kv, n_tp, kv_local, group, math.log2(math.e) / math.sqrt(HEAD // MAPS)
        ),
        out_shape=pltpu.VMEM((batch, depth // n_tp), BF16),
        in_specs=[hbm] * 16,
        out_specs=pl.BlockSpec(memory_space=pltpu.VMEM),
        scratch_shapes=[
            pltpu.VMEM(tokens.shape, BF16),
            pltpu.VMEM((1, depth), F32),
            pltpu.VMEM((1, depth), F32),
            pltpu.VMEM((1, depth), F32),
            pltpu.VMEM((1, kv_local * group), F32),
            pltpu.VMEM((1, HEAD), F32),
            pltpu.VMEM((depth, COL_GROUPS * cw), BF16),
            pltpu.VMEM((depth, COL_GROUPS * cw), BF16),
            pltpu.VMEM(first_down.shape, BF16),
            pltpu.VMEM(w_query.shape, BF16),
            pltpu.VMEM((pairs, length, 2 * LANES), BF16),
            pltpu.VMEM((pairs, 2 * LANES, length), BF16),
            pltpu.VMEM((pairs, length, 2 * LANES), BF16),
            pltpu.VMEM(w_out.shape, BF16),
            pltpu.VMEM((depth, COL_GROUPS * cw), BF16),
            pltpu.VMEM((depth, COL_GROUPS * cw), BF16),
            pltpu.VMEM(second_down.shape, BF16),
            pltpu.VMEM((n_tp,) + tokens.shape, BF16),
            *ffn_buffers,
            *tp_buffers,
            pltpu.VMEM((q_tiles, TILE, LANES), BF16),
            pltpu.VMEM((n_kv - 1, q_tiles, TILE, LANES), BF16),
            pltpu.VMEM((pairs, 2 * TILE, 2 * LANES), BF16),
            pltpu.VMEM((pairs, TILE, LANES), BF16),
            pltpu.VMEM((n_kv - 1, pairs, TILE, LANES), BF16),
            pltpu.VMEM((2, TILE, LANES), BF16),
            pltpu.VMEM((n_kv - 1, 2, TILE, LANES), BF16),
            pltpu.VMEM((2 * pairs, pairs // 2 * LANES), BF16),
            pltpu.VMEM((pairs * TILE, LANES), F32),
            *tp_buffers,
            *ffn_buffers,
            pltpu.VMEM((n_tp, batch, own_width), BF16),
            pltpu.VMEM((n_tp - 1, batch, own_width), BF16),
            pltpu.SemaphoreType.DMA((6,)),
            pltpu.SemaphoreType.DMA((7 + kv_local * group,)),
            pltpu.SemaphoreType.DMA((8,)),
            pltpu.SemaphoreType.DMA((11,)),
            pltpu.SemaphoreType.DMA((3,)),
            pltpu.SemaphoreType.DMA((n_kv - 1,)),
            pltpu.SemaphoreType.DMA((n_kv - 1,)),
            pltpu.SemaphoreType.DMA((n_tp - 1,)),
            pltpu.SemaphoreType.DMA((n_tp - 1,)),
            pltpu.SemaphoreType.DMA((n_tp - 1,)),
            pltpu.SemaphoreType.DMA((4,)),
            pltpu.SemaphoreType.DMA((4,)),
        ],
        compiler_params=pltpu.CompilerParams(
            collective_id=1, has_side_effects=True, vmem_limit_bytes=VMEM_LIMIT
        ),
    )(
        tokens, first_gain.reshape(1, -1), mix_gain.reshape(1, -1), second_gain.reshape(1, -1),
        map_weight.reshape(1, -1), head_gain.reshape(1, -1),
        first_gate, first_up, first_down, w_query, key_cache, value_cache, w_out,
        second_gate, second_up, second_down,
    )


def solution(mesh):
    placed = (
        P(None, ("kv", "tp")),
        P("kv"),
        P("kv", "tp"),
        P("kv", "tp"),
        P("tp", "kv"),
        P("kv"),
        P("kv", "tp"),
        P(None, "kv", "tp"),
        P(None, "kv", "tp"),
        P("tp"),
        P(),
        P("tp", "kv"),
        P("kv"),
        P("kv", "tp"),
        P("kv", "tp"),
        P("tp", "kv"),
    )
    return jax.shard_map(
        functools.partial(on_device, mesh.shape["kv"], mesh.shape["tp"]),
        mesh=mesh,
        in_specs=placed,
        out_specs=P(None, ("kv", "tp")),
        check_vma=False,
    )
```
